128 devices in a mesh: sp: 16 (over z, y), tp: 8 (over x, core).
Axes of the slice: x: 4, y: 4, z: 4, core: 2. Of those that a mesh axis runs over, the one named last changes fastest.
Arguments:
- tokens: bfloat16 [12288, 2048], P('sp', 'tp'), may hold values from -6 to 6
- norm_gain: float32 [2048], replicated, may hold values from 0.1 to 1.9
- w_query: bfloat16 [2048, 2048], P(None, 'tp'), may hold values from -4 to 4
- w_key: bfloat16 [2048, 2048], P(None, 'tp'), may hold values from -4 to 4
- w_value: bfloat16 [2048, 2048], P(None, 'tp'), may hold values from -0.125 to 0.125
- w_outer: bfloat16 [2048, 2048], P(None, 'tp'), may hold values from -0.125 to 0.125
- w_inner: bfloat16 [2048, 2048], P(None, 'tp'), may hold values from -0.125 to 0.125
- w_signal: bfloat16 [2048, 2048], P(None, 'tp'), may hold values from -0.125 to 0.125
- conv_taps: bfloat16 [3, 2048], P(None, 'tp'), may hold values from -3.5 to 3.5
- lambdas: float32 [8], P('tp'), may hold values from 0.3 to 0.8
- head_gain: float32 [256], replicated, may hold values from 0.1 to 1.9
- attend_proj: bfloat16 [2048, 2048], P('tp'), may hold values from -0.125 to 0.125
- convolve_proj: bfloat16 [2048, 2048], P('tp'), may hold values from -0.125 to 0.125
Outputs:
- mixed: bfloat16 [12288, 2048], P(('sp', 'tp'))
- row_lse: float32 [12288, 16], P('sp', 'tp')
The draws below stay inside these ranges and needn't reach their ends.
All inputs are finite; a program needn't handle non-finite values.
Results may differ from the reference program's by a relative error of at most 0.015.
Values may be sent and summed in bfloat16 or wider, within the bound.
A program may use at most 128 MiB of HBM per device.

```python
import math
import jax
import jax.numpy as jnp
from jax import lax

D = 2048
HEADS = 8
HEAD_DIM = 128
CONV = 2048
TOK_DEV = 768
TOKENS = 12288
N_TP = 8


def query_key_pair(key):
    width = 2 * HEADS * HEAD_DIM
    spread = 1.3 / math.sqrt(D)
    key_part = jax.random.normal(jax.random.fold_in(key, 701), (D, width), jnp.float32) * spread
    noise_part = jax.random.normal(jax.random.fold_in(key, 702), (D, width), jnp.float32) * spread
    query_part = noise_part
    return (jnp.clip(query_part, -4.0, 4.0), jnp.clip(key_part, -4.0, 4.0))


def draw_w_query(key, part):
    return query_key_pair(key)[0].astype(jnp.bfloat16)


def draw_w_key(key, part):
    return query_key_pair(key)[1].astype(jnp.bfloat16)


def level_of(rng, dims, cuts, least, top_value):
    def one(position, parts):
        heights = jax.random.uniform(jax.random.fold_in(jax.random.fold_in(rng, 6), position), (parts,), jnp.float32, least / len(cuts), top_value / len(cuts))
        return jnp.repeat(jnp.exp(heights), dims[position] // parts).reshape((-1,) + (1,) * (len(dims) - position - 1))

    loudness = one(*cuts[0])
    for cut in cuts[1:]:
        loudness = loudness * one(*cut)
    return loudness


def bell_draw(rng, shape, scale, limit, pieces=(), kind=jnp.bfloat16):
    level = level_of(rng, shape, pieces, -0.22, 0.18) if pieces else 1.0
    entries = jax.random.normal(rng, shape, jnp.float32) * scale * level
    return jnp.minimum(jnp.maximum(entries, -limit), limit).astype(kind)


def setup_inputs(seed: int = 0) -> dict:
    keys = jax.random.split(jax.random.key(seed), 14)
    return {
        "tokens": bell_draw(keys[0], (TOKENS, D), 1.0, 6.0, ((0, 16), (1, 8))),
        "norm_gain": jnp.clip(1.0 + 0.18 * jax.random.normal(keys[1], (D,), jnp.float32), 0.1, 1.9),
        "w_query": draw_w_query(jax.random.fold_in(keys[13], 71), 0),
        "w_key": draw_w_key(jax.random.fold_in(keys[13], 71), 0),
        "w_value": bell_draw(keys[4], (D, 2 * HEADS * HEAD_DIM), D ** -0.5, 0.125, ((1, 8),)),
        "w_outer": bell_draw(keys[5], (D, CONV), D ** -0.5, 0.125, ((1, 8),)),
        "w_inner": bell_draw(keys[6], (D, CONV), D ** -0.5, 0.125, ((1, 8),)),
        "w_signal": bell_draw(keys[7], (D, CONV), D ** -0.5, 0.125, ((1, 8),)),
        "conv_taps": bell_draw(keys[8], (3, CONV), 3 ** -0.5, 3.5, ((1, 8),)),
        "lambdas": jnp.clip(0.3 + 0.5 * jax.random.uniform(keys[9], (HEADS,), jnp.float32) ** level_of(keys[9], (HEADS,), ((0, 8),), -0.2, 0.2), 0.3, 0.8),
        "head_gain": jnp.clip(1.0 + 0.18 * jax.random.normal(keys[10], (2 * HEAD_DIM,), jnp.float32), 0.1, 1.9),
        "attend_proj": bell_draw(keys[11], (2 * HEADS * HEAD_DIM, D), (2 * HEADS * HEAD_DIM) ** -0.5, 0.125, ((0, 8),)),
        "convolve_proj": bell_draw(keys[12], (CONV, D), CONV ** -0.5, 0.125, ((0, 8),)),
    }


ROPE_BASE = 500000.0
NORM_EPS = 1e-05
HEAD_KEEP = 0.8
MASKED = -1e+30

def rotate(values_in, positions):
    half_width = values_in.shape[-1] // 2
    inverse = ROPE_BASE ** (-jnp.arange(half_width, dtype=jnp.float32) * 2.0 / values_in.shape[-1])
    angles = positions.astype(jnp.float32)[:, None] * inverse[None, :]
    cosine = jnp.cos(angles)[:, None, :]
    sine_part = jnp.sin(angles)[:, None, :]
    first_half = values_in[..., :half_width]
    second_half = values_in[..., half_width:]
    return jnp.concatenate([first_half * cosine - second_half * sine_part, second_half * cosine + first_half * sine_part], axis=-1)

def reference(tokens, norm_gain, w_query, w_key, w_value, w_outer, w_inner, w_signal, conv_taps, lambdas, head_gain, attend_proj, convolve_proj):
    row_count = tokens.shape[0]
    widened = tokens.astype(jnp.float32)
    scaled = (widened * norm_gain[None, :]).astype(jnp.bfloat16)
    inv_rms = lax.rsqrt(lax.optimization_barrier(jnp.mean(widened * widened, axis=1, keepdims=True)) + NORM_EPS)

    def project(weight):
        return inv_rms * jnp.dot(scaled, weight, preferred_element_type=jnp.float32)
    positions = jnp.arange(row_count, dtype=jnp.int32)
    queries = rotate(project(w_query).reshape(row_count, 2 * HEADS, HEAD_DIM), positions).astype(jnp.bfloat16)
    key_rows = rotate(project(w_key).reshape(row_count, 2 * HEADS, HEAD_DIM), positions).astype(jnp.bfloat16)
    value_rows = project(w_value).astype(jnp.bfloat16).reshape(row_count, HEADS, 2 * HEAD_DIM)
    block_count = row_count // TOK_DEV
    key_places = jnp.arange(row_count, dtype=jnp.int32)
    attended_heads = []
    lse_heads = []
    for head_index in range(HEADS):
        head_query = queries[:, 2 * head_index:2 * head_index + 2, :].astype(jnp.float32)
        head_key = key_rows[:, 2 * head_index:2 * head_index + 2, :].astype(jnp.float32)
        head_value = value_rows[:, head_index, :].astype(jnp.float32)
        head_lambda = lambdas[head_index]

        def one_block(block_index):
            first_row = block_index * TOK_DEV
            query_block = lax.dynamic_slice_in_dim(head_query, first_row, TOK_DEV, 0)
            scores = jnp.einsum('qjd,kjd->jqk', query_block, head_key) * HEAD_DIM ** (-0.5)
            query_places = first_row + jnp.arange(TOK_DEV, dtype=jnp.int32)
            allowed = key_places[None, :] <= query_places[:, None]
            scores = jnp.where(allowed[None], scores, MASKED)
            running_max = lax.optimization_barrier(jnp.max(scores, axis=2, keepdims=True))
            lifted = jnp.exp(scores - running_max)
            weight_sum = lax.optimization_barrier(jnp.sum(lifted, axis=2, keepdims=True))
            weights = lax.optimization_barrier((lifted / weight_sum).astype(jnp.bfloat16))
            mixed_pair = jnp.einsum('jqk,ke->jqe', weights.astype(jnp.float32), head_value)
            difference = mixed_pair[0] - head_lambda * mixed_pair[1]
            scale_back = lax.rsqrt(lax.optimization_barrier(jnp.mean(difference * difference, axis=1, keepdims=True)) + NORM_EPS)
            normed = (difference * scale_back * head_gain[None, :] * HEAD_KEEP).astype(jnp.bfloat16)
            log_sum = jnp.transpose((running_max + jnp.log(weight_sum))[:, :, 0], (1, 0))
            return (normed, log_sum)
        normed_blocks, lse_blocks = lax.map(one_block, jnp.arange(block_count, dtype=jnp.int32))
        attended_heads.append(normed_blocks.reshape(row_count, 2 * HEAD_DIM))
        lse_heads.append(lse_blocks.reshape(row_count, 2))
    attended = jnp.concatenate(attended_heads, axis=1)
    row_lse = jnp.concatenate(lse_heads, axis=1)
    product = project(w_inner) * project(w_signal)
    padded = jnp.concatenate([jnp.zeros((2, CONV), jnp.float32), product], axis=0)
    tap_values = conv_taps.astype(jnp.float32)
    smoothed = tap_values[0] * padded[:-2] + tap_values[1] * padded[1:-1] + tap_values[2] * padded[2:]
    convolved = (project(w_outer) * smoothed).astype(jnp.bfloat16)
    head_columns = HEADS // N_TP * 2 * HEAD_DIM
    channel_columns = CONV // N_TP
    summed = jnp.zeros((row_count, D), jnp.float32)
    for group_index in range(N_TP):
        head_lo = group_index * head_columns
        chan_lo = group_index * channel_columns
        partial_value = jnp.dot(attended[:, head_lo:head_lo + head_columns], attend_proj[head_lo:head_lo + head_columns], preferred_element_type=jnp.float32)
        partial_value = partial_value + jnp.dot(convolved[:, chan_lo:chan_lo + channel_columns], convolve_proj[chan_lo:chan_lo + channel_columns], preferred_element_type=jnp.float32)
        rounded = lax.optimization_barrier(partial_value.astype(jnp.bfloat16))
        summed = summed + rounded.astype(jnp.float32)
    return (summed.astype(jnp.bfloat16), row_lse)
```

```python
import functools

import jax
import jax.numpy as jnp
import numpy as np
from jax import lax
from jax.experimental import pallas as pl
from jax.experimental.pallas import tpu as pltpu
from jax.sharding import PartitionSpec as P

MESH = pl.DeviceIdType.MESH
BF = jnp.bfloat16
F32 = jnp.float32
ROPE_BASE = 500000.0
NORM_EPS = 1e-05
HEAD_KEEP = 0.8
MASKED = -1e30
LOG2E = float(np.log2(np.e))
LN2 = float(np.log(2.0))
NZ, NY, NX = 4, 4, 4
ROWS = 768
HD = 128
VD = 256
CH = 256
NCH = ROWS // CH
HALF = ROWS // 2
BLK = 96


def vmem():
    return pl.BlockSpec(memory_space=pltpu.VMEM)


def hbm():
    return pl.BlockSpec(memory_space=pl.ANY)


def remote(src, dst, ssem, rsem, dev):
    return pltpu.make_async_remote_copy(
        src_ref=src, dst_ref=dst, send_sem=ssem, recv_sem=rsem, device_id=dev, device_id_type=MESH
    )


def greet(devs):
    barrier = pltpu.get_barrier_semaphore()
    for dev in devs:
        pl.semaphore_signal(barrier, inc=1, device_id=dev, device_id_type=MESH)
    pl.semaphore_wait(barrier, len(devs))


def project_kernel(
    tok, gain, wq, wk, wv, wo, wi, ws, taps, rc, rs, oc, os_,
    q_out, kv_out, conv_out,
    xbuf, sc, wbuf, prod, outer, wsem, ssem, rsem, bsem,
):
    sp = lax.axis_index("sp")
    tp = lax.axis_index("tp")
    x = tp // 2
    c = tp % 2
    right = lax.rem(x + 1, NX) * 2 + c
    left = lax.rem(x + 3, NX) * 2 + c
    opp = lax.rem(x + 2, NX) * 2 + c
    mate = x * 2 + (1 - c)
    dr, dl, dm = (sp, right), (sp, left), (sp, mate)
    dn, dp = (lax.rem(sp + 1, NZ * NY), tp), (lax.rem(sp + NZ * NY - 1, NZ * NY), tp)
    weights = (wk, wv, wq, wi, ws, wo)
    wcopies = [pltpu.make_async_copy(w, wbuf.at[i], wsem.at[i]) for i, w in enumerate(weights)]
    for copy in wcopies:
        copy.start()
    greet([dr, dl, dm, dn, dp])

    def rows_of(k, part):
        if part is None:
            return pl.ds(k * CH, CH)
        return pl.ds(k * CH + part * (CH // 2), CH // 2)

    def own(k, kind, dev):
        return remote(
            tok.at[rows_of(k, None)], xbuf.at[tp, rows_of(k, None)],
            ssem.at[k, kind], rsem.at[k, kind], dev,
        )

    def pass_on(k, kind, block, part, dev):
        ref = xbuf.at[block, rows_of(k, part)]
        return remote(ref, ref, ssem.at[k, kind], rsem.at[k, kind], dev)

    sent = []

    def go(copy):
        copy.start()
        sent.append(copy)

    def send_own(k):
        go(own(k, 0, dr))
        go(own(k, 1, dl))
        go(own(k, 2, dm))

    def near(k):
        own(k, 0, dr).wait_recv()
        go(pass_on(k, 3, left, 0, dr))
        go(pass_on(k, 5, left, None, dm))
        own(k, 1, dl).wait_recv()
        go(pass_on(k, 4, right, 1, dl))
        go(pass_on(k, 6, right, None, dm))

    def far(k):
        pass_on(k, 3, left, 0, dr).wait_recv()
        go(pass_on(k, 7, opp, 0, dm))
        pass_on(k, 4, right, 1, dl).wait_recv()
        go(pass_on(k, 8, opp, 1, dm))

    def mates(k):
        own(k, 2, dm).wait_recv()
        pass_on(k, 5, left, None, dm).wait_recv()
        pass_on(k, 6, right, None, dm).wait_recv()
        pass_on(k, 7, opp, 0, dm).wait_recv()
        pass_on(k, 8, opp, 1, dm).wait_recv()

    send_own(0)
    send_own(1)
    xbuf[tp] = tok[...]
    co = oc[pl.ds(sp, 1), :]
    so = os_[pl.ds(sp, 1), :]

    def turn(v, k):
        c_r = rc[rows_of(k, None), :]
        s_r = rs[rows_of(k, None), :]
        cosine = co * c_r - so * s_r
        sine = so * c_r + co * s_r
        lane = lax.broadcasted_iota(jnp.int32, (CH, HD), 1)
        sine = jnp.where(lane < HD // 2, -sine, sine)
        parts = []
        for j in range(2):
            t = v[:, j * HD:(j + 1) * HD]
            parts.append(t * cosine + pltpu.roll(t, HD // 2, 1) * sine)
        return jnp.concatenate(parts, axis=1)

    def compute(k):
        rows = rows_of(k, None)
        square = jnp.zeros((CH, HD), F32)
        for b in range(2 * NX):
            xb = xbuf[b, rows, :].astype(F32)
            square += xb[:, :HD] * xb[:, :HD] + xb[:, HD:] * xb[:, HD:]
            sc[:, b * 256:(b + 1) * 256] = (xb * gain[:, b * 256:(b + 1) * 256]).astype(BF)
        total = jnp.sum(square, axis=1, keepdims=True)
        inv = lax.rsqrt(total / (2 * NX * 256) + NORM_EPS)

        def project(i):
            return inv * jnp.dot(sc[...], wbuf[i], preferred_element_type=F32)

        kv_out[rows, 0:VD] = turn(project(0), k).astype(BF)
        kv_out[rows, VD:2 * VD] = project(1).astype(BF)
        q_out[rows, :] = (turn(project(2), k) * (LOG2E * HD ** -0.5)).astype(BF)
        prod[pl.ds(8 + k * CH, CH), :] = project(3) * project(4)
        outer[rows, :] = project(5)

    near(0)
    near(1)
    send_own(2)
    far(0)
    mates(0)
    for copy in wcopies:
        copy.wait()
    compute(0)
    near(2)
    far(1)
    mates(1)
    compute(1)
    far(2)
    mates(2)
    compute(2)
    border = remote(
        prod.at[pl.ds(ROWS, 8)], prod.at[pl.ds(0, 8)], bsem.at[0], bsem.at[1], dn
    )
    border.start()
    border.wait_recv()
    border.wait_send()

    @pl.when(sp == 0)
    def _():
        prod[0:8, :] = jnp.zeros((8, 256), F32)

    tv = taps[...].astype(F32)
    smoothed = (
        tv[0:1] * prod[6:6 + ROWS, :] + tv[1:2] * prod[7:7 + ROWS, :] + tv[2:3] * prod[8:8 + ROWS, :]
    )
    conv_out[...] = (outer[...] * smoothed).astype(BF)
    for copy in sent:
        copy.wait_send()


def attend_kernel(
    lam, hgain, q_ref, kv_ref,
    att_ref, lse_ref,
    qb, kvb, m_ref, l_ref, acc, lt, stats, dbuf, relay, fin,
    qss, qrs, kss, krs, tss, trs, dss, drs,
):
    sp = lax.axis_index("sp")
    tp = lax.axis_index("tp")
    z = sp // NY
    y = sp % NY
    yr, yl, yo = lax.rem(y + 1, NY), lax.rem(y + 3, NY), lax.rem(y + 2, NY)
    zr, zl, zo = lax.rem(z + 1, NZ), lax.rem(z + 3, NZ), lax.rem(z + 2, NZ)
    dyr, dyl, dyo = (z * NY + yr, tp), (z * NY + yl, tp), (z * NY + yo, tp)
    dzr, dzl = (zr * NY + y, tp), (zl * NY + y, tp)
    greet([dyr, dyl, dyo, dzr, dzl])
    sent = []

    def go(copy):
        copy.start()
        sent.append(copy)

    def gather(src, buf, me, left, right, ss, rs, d_r, d_l):
        def part(h):
            return pl.ds(h * HALF, HALF)

        def own(h, kind, dev):
            return remote(src.at[part(h)], buf.at[me, part(h)], ss.at[kind], rs.at[kind], dev)

        def pass_on(block, h, kind, dev):
            ref = buf.at[block, part(h)]
            return remote(ref, ref, ss.at[kind], rs.at[kind], dev)

        copies = [
            own(0, 0, d_r), own(1, 1, d_r), own(1, 2, d_l), own(0, 3, d_l),
            pass_on(left, 0, 4, d_r), pass_on(right, 1, 5, d_l),
        ]
        for i in (0, 2, 1, 3):
            go(copies[i])

        def first():
            copies[0].wait_recv()
            go(copies[4])
            copies[2].wait_recv()
            go(copies[5])

        def second():
            copies[1].wait_recv()
            copies[3].wait_recv()

        def third():
            copies[4].wait_recv()
            copies[5].wait_recv()

        return first, second, third

    k1, k2, k3 = gather(kv_ref, kvb, z, zl, zr, kss, krs, dzr, dzl)
    q1, q2, q3 = gather(q_ref, qb, y, yl, yr, qss, qrs, dyr, dyl)
    qb[y] = q_ref[...]
    kvb[z] = kv_ref[...]
    m_ref[...] = jnp.full(m_ref.shape, MASKED, F32)
    l_ref[...] = jnp.zeros(l_ref.shape, F32)
    acc[...] = jnp.zeros(acc.shape, F32)

    def scores(qi, kj, r, tq, nk, j):
        q = qb[qi, pl.ds(r, tq), j * HD:(j + 1) * HD]
        k = kvb[kj, 0:nk, j * HD:(j + 1) * HD]
        return lax.dot_general(q, k, (((1,), (1,)), ((), ())), preferred_element_type=F32)

    def absorb(qi, kj, r, tq, nk, j, s):
        rows = pl.ds(r, tq)
        before = m_ref[j, qi, rows, :]
        now = jnp.maximum(before, jnp.max(s, axis=1, keepdims=True))
        fade = jnp.exp2(before - now)
        p = jnp.exp2(s - jnp.concatenate([now] * (nk // HD), axis=1))
        total = l_ref[j, qi, rows, :] * fade
        for i in range(nk // HD):
            total = total + p[:, i * HD:(i + 1) * HD]
        l_ref[j, qi, rows, :] = total
        m_ref[j, qi, rows, :] = now
        v = kvb[kj, 0:nk, VD:2 * VD]
        acc[j, qi, rows, :] = acc[j, qi, rows, :] * jnp.concatenate([fade] * 2, axis=1) + jnp.dot(
            p.astype(BF), v, preferred_element_type=F32
        )

    def full(qi, kj):
        s0 = scores(qi, kj, 0, ROWS, ROWS, 0)
        s1 = scores(qi, kj, 0, ROWS, ROWS, 1)
        absorb(qi, kj, 0, ROWS, ROWS, 0, s0)
        absorb(qi, kj, 0, ROWS, ROWS, 1, s1)

    def diagonal():
        for t in range(NCH):
            nk = (t + 1) * CH
            row = lax.broadcasted_iota(jnp.int32, (CH, nk), 0) + t * CH
            col = lax.broadcasted_iota(jnp.int32, (CH, nk), 1)
            ss = [scores(y, z, t * CH, CH, nk, j) for j in range(2)]
            for j in range(2):
                absorb(y, z, t * CH, CH, nk, j, jnp.where(col <= row, ss[j], MASKED))

    diagonal()
    q1()
    k1()
    q2()
    q3()

    def own_kv(i, _):
        qi = lax.rem(y + 1 + i, NY)

        @pl.when(qi > y)
        def _():
            full(qi, z)

        return 0

    lax.fori_loop(0, NY - 1, own_kv, 0)
    k2()

    def sweep(kj, least):
        @pl.when(z >= least)
        def _():
            def step(i, _):
                full(i, kj)
                return 0

            lax.fori_loop(0, NY, step, 0)

    sweep(zl, 1)
    sweep(zr, 3)
    k3()
    sweep(zo, 2)

    lane = lax.broadcasted_iota(jnp.int32, (ROWS, HD), 1)
    table = jnp.full((ROWS, HD), MASKED, F32)
    for qi in range(NY):
        for j in range(2):
            total = jnp.sum(l_ref[j, qi], axis=1, keepdims=True)
            lse = m_ref[j, qi] + jnp.log2(jnp.maximum(total, 1e-37))
            table = jnp.where(lane == 2 * qi + j, lse, table)
    stats[y] = jnp.transpose(table)[0:8, :]
    exchange = [
        remote(stats.at[y], stats.at[y], tss.at[i], trs.at[i], dev)
        for i, dev in enumerate((dyr, dyl, dyo))
    ]
    for copy in exchange:
        go(copy)
    for copy in exchange:
        copy.wait_recv()
    parts = [stats[i] for i in range(NY)]
    peak = jnp.maximum(jnp.maximum(parts[0], parts[1]), jnp.maximum(parts[2], parts[3]))
    whole = peak + jnp.log2(sum(jnp.exp2(p - peak) for p in parts))
    lt[...] = jnp.transpose(jnp.concatenate([whole, jnp.zeros((HD - 8, ROWS), F32)], axis=0))

    lam_v = lam[...]
    step_rows = 128

    def pick(rows, qi, j):
        lanes = lax.broadcasted_iota(jnp.int32, (step_rows, HD), 1)
        return jnp.sum(jnp.where(lanes == 2 * qi + j, lt[rows, :], 0.0), axis=1, keepdims=True)

    def share(rows, qi):
        outs = []
        for j in range(2):
            f = jnp.exp2(m_ref[j, qi, rows, :] - pick(rows, qi, j))
            outs.append(acc[j, qi, rows, :] * jnp.concatenate([f] * 2, axis=1))
        return outs[0] - lam_v * outs[1]

    def shares(qi):
        def one(i, _):
            rows = pl.ds(pl.multiple_of(i * step_rows, step_rows), step_rows)
            dbuf[qi, rows, :] = share(rows, qi).astype(BF)
            return 0

        lax.fori_loop(0, ROWS // step_rows, one, 0)

    h0, h1 = pl.ds(0, HALF), pl.ds(HALF, HALF)
    far = [
        remote(dbuf.at[yo, h0], relay.at[0], dss.at[0], drs.at[0], dyr),
        remote(dbuf.at[yo, h1], relay.at[1], dss.at[1], drs.at[1], dyl),
    ]
    near = [
        remote(dbuf.at[yr, h1], fin.at[0, h1], dss.at[2], drs.at[2], dyr),
        remote(dbuf.at[yl, h0], fin.at[1, h0], dss.at[3], drs.at[3], dyl),
        remote(dbuf.at[yr, h0], fin.at[0, h0], dss.at[4], drs.at[4], dyr),
        remote(dbuf.at[yl, h1], fin.at[1, h1], dss.at[5], drs.at[5], dyl),
    ]
    shares(yo)
    go(far[0])
    go(far[1])
    shares(yr)
    shares(yl)
    go(near[0])
    go(near[1])
    far[0].wait_recv()
    dbuf[yr, h0, :] = (dbuf[yr, h0, :].astype(F32) + relay[0].astype(F32)).astype(BF)
    go(near[2])
    far[1].wait_recv()
    dbuf[yl, h1, :] = (dbuf[yl, h1, :].astype(F32) + relay[1].astype(F32)).astype(BF)
    go(near[3])
    for copy in near:
        copy.wait_recv()

    def last(i, _):
        rows = pl.ds(pl.multiple_of(i * step_rows, step_rows), step_rows)
        d = share(rows, y) + fin[0, rows, :].astype(F32) + fin[1, rows, :].astype(F32)
        back = lax.rsqrt(jnp.mean(d * d, axis=1, keepdims=True) + NORM_EPS)
        att_ref[rows, :] = (d * back * hgain[...] * HEAD_KEEP).astype(BF)
        lse_ref[rows, 0:1] = pick(rows, y, 0) * LN2
        lse_ref[rows, 1:2] = pick(rows, y, 1) * LN2
        return 0

    lax.fori_loop(0, ROWS // step_rows, last, 0)
    for copy in sent:
        copy.wait_send()


def merge_kernel(
    att, conv, ap, cp,
    out,
    part, precv, relay, fin, apb, cpb,
    wsem, pss, prs, rss, rrs,
):
    sp = lax.axis_index("sp")
    tp = lax.axis_index("tp")
    x = tp // 2
    c = tp % 2
    xr, xl, xo = lax.rem(x + 1, NX), lax.rem(x + 3, NX), lax.rem(x + 2, NX)
    dr, dl, dm = (sp, xr * 2 + c), (sp, xl * 2 + c), (sp, x * 2 + (1 - c))
    loads = [pltpu.make_async_copy(ap, apb, wsem.at[0]), pltpu.make_async_copy(cp, cpb, wsem.at[1])]
    for copy in loads:
        copy.start()
    greet([dr, dl, dm])
    for copy in loads:
        copy.wait()
    sent = []

    def go(copy):
        copy.start()
        sent.append(copy)

    cols = 512
    order = (xo, xr, xl, x)
    mates = [
        remote(part.at[xx * 2 + (1 - c)], precv.at[xx], pss.at[i], prs.at[i], dm)
        for i, xx in enumerate(order)
    ]

    def compute(xx):
        rows = pl.ds(pl.multiple_of(xx * (2 * BLK), 2 * BLK), 2 * BLK)
        a = att[rows, :]
        b = conv[rows, :]
        for n in range(2048 // cols):
            cs = slice(n * cols, (n + 1) * cols)
            p = jnp.dot(a, apb[:, cs], preferred_element_type=F32) + jnp.dot(
                b, cpb[:, cs], preferred_element_type=F32
            )
            p = p.astype(BF)
            part[xx * 2, :, cs] = p[:BLK]
            part[xx * 2 + 1, :, cs] = p[BLK:]

    def join(xx, rows, extra):
        t = part[xx * 2 + c, rows, :].astype(F32) + precv[xx, rows, :].astype(F32)
        if extra is not None:
            t = t + extra[...].astype(F32)
        part[xx * 2 + c, rows, :] = t.astype(BF)

    h0, h1 = pl.ds(0, BLK // 2), pl.ds(BLK // 2, BLK // 2)
    io, ir, il = xo * 2 + c, xr * 2 + c, xl * 2 + c
    far = [
        remote(part.at[io, h0], relay.at[0], rss.at[0], rrs.at[0], dr),
        remote(part.at[io, h1], relay.at[1], rss.at[1], rrs.at[1], dl),
    ]
    near = [
        remote(part.at[ir, h1], fin.at[0, h1], rss.at[2], rrs.at[2], dr),
        remote(part.at[il, h0], fin.at[1, h0], rss.at[3], rrs.at[3], dl),
        remote(part.at[ir, h0], fin.at[0, h0], rss.at[4], rrs.at[4], dr),
        remote(part.at[il, h1], fin.at[1, h1], rss.at[5], rrs.at[5], dl),
    ]
    compute(xo)
    go(mates[0])
    compute(xr)
    go(mates[1])
    mates[0].wait_recv()
    join(xo, h0, None)
    join(xo, h1, None)
    go(far[0])
    go(far[1])
    compute(xl)
    go(mates[2])
    mates[1].wait_recv()
    join(xr, h1, None)
    go(near[0])
    compute(x)
    go(mates[3])
    mates[2].wait_recv()
    join(xl, h0, None)
    go(near[1])
    far[0].wait_recv()
    join(xr, h0, relay.at[0])
    go(near[2])
    far[1].wait_recv()
    join(xl, h1, relay.at[1])
    go(near[3])
    mates[3].wait_recv()
    for copy in near:
        copy.wait_recv()
    out[...] = (
        part[tp].astype(F32) + precv[x].astype(F32) + fin[0].astype(F32) + fin[1].astype(F32)
    ).astype(BF)
    for copy in sent:
        copy.wait_send()


def tables():
    inverse = ROPE_BASE ** (-np.arange(HD // 2, dtype=np.float64) * 2.0 / HD)
    inverse = inverse.astype(np.float32).astype(np.float64)
    inverse = np.concatenate([inverse, inverse])
    local = np.arange(ROWS)[:, None] * inverse[None, :]
    offset = (np.arange(NZ * NY) * ROWS)[:, None] * inverse[None, :]
    return [f(a).astype(np.float32) for a in (local, offset) for f in (np.cos, np.sin)]


def params(cid):
    return pltpu.CompilerParams(
        collective_id=cid, has_side_effects=True, vmem_limit_bytes=60 * 2 ** 20
    )


DMA = pltpu.SemaphoreType.DMA


def per_device(
    tokens, norm_gain, w_query, w_key, w_value, w_outer, w_inner, w_signal,
    conv_taps, lambdas, head_gain, attend_proj, convolve_proj,
):
    rc, rs, oc, os_ = tables()
    q, kv, conv = pl.pallas_call(
        project_kernel,
        out_shape=(
            jax.ShapeDtypeStruct((ROWS, VD), BF),
            jax.ShapeDtypeStruct((ROWS, 2 * VD), BF),
            jax.ShapeDtypeStruct((ROWS, 256), BF),
        ),
        in_specs=[vmem(), vmem()] + [hbm()] * 6 + [vmem()] * 5,
        out_specs=(vmem(), vmem(), vmem()),
        scratch_shapes=[
            pltpu.VMEM((2 * NX, ROWS, 256), BF),
            pltpu.VMEM((CH, 2048), BF),
            pltpu.VMEM((6, 2048, 256), BF),
            pltpu.VMEM((ROWS + 8, 256), F32),
            pltpu.VMEM((ROWS, 256), F32),
            DMA((6,)), DMA((NCH, 9)), DMA((NCH, 9)), DMA((2,)),
        ],
        compiler_params=params(1),
        name="project",
    )(
        tokens, norm_gain.reshape(1, -1), w_query, w_key, w_value, w_outer, w_inner, w_signal,
        conv_taps, rc, rs, oc, os_,
    )
    att, lse = pl.pallas_call(
        attend_kernel,
        out_shape=(
            jax.ShapeDtypeStruct((ROWS, VD), BF),
            jax.ShapeDtypeStruct((ROWS, 2), F32),
        ),
        in_specs=[vmem()] * 4,
        out_specs=(vmem(), vmem()),
        scratch_shapes=[
            pltpu.VMEM((NY, ROWS, VD), BF),
            pltpu.VMEM((NZ, ROWS, 2 * VD), BF),
            pltpu.VMEM((2, NY, ROWS, HD), F32),
            pltpu.VMEM((2, NY, ROWS, HD), F32),
            pltpu.VMEM((2, NY, ROWS, VD), F32),
            pltpu.VMEM((ROWS, HD), F32),
            pltpu.VMEM((NY, 8, ROWS), F32),
            pltpu.VMEM((NY, ROWS, VD), BF),
            pltpu.VMEM((2, HALF, VD), BF),
            pltpu.VMEM((2, ROWS, VD), BF),
            DMA((6,)), DMA((6,)), DMA((6,)), DMA((6,)), DMA((3,)), DMA((3,)), DMA((6,)), DMA((6,)),
        ],
        compiler_params=params(2),
        name="attend",
    )(lambdas.reshape(1, 1), head_gain.reshape(1, -1), q, kv)
    mixed = pl.pallas_call(
        merge_kernel,
        out_shape=jax.ShapeDtypeStruct((BLK, 2048), BF),
        in_specs=[vmem(), vmem(), hbm(), hbm()],
        out_specs=vmem(),
        scratch_shapes=[
            pltpu.VMEM((2 * NX, BLK, 2048), BF),
            pltpu.VMEM((NX, BLK, 2048), BF),
            pltpu.VMEM((2, BLK // 2, 2048), BF),
            pltpu.VMEM((2, BLK, 2048), BF),
            pltpu.VMEM((256, 2048), BF),
            pltpu.VMEM((256, 2048), BF),
            DMA((2,)), DMA((4,)), DMA((4,)), DMA((6,)), DMA((6,)),
        ],
        compiler_params=params(3),
        name="merge",
    )(att, conv, attend_proj, convolve_proj)
    return mixed, lse


def solution(mesh):
    return jax.shard_map(
        per_device,
        mesh=mesh,
        in_specs=(
            P("sp", "tp"), P(), P(None, "tp"), P(None, "tp"), P(None, "tp"), P(None, "tp"),
            P(None, "tp"), P(None, "tp"), P(None, "tp"), P("tp"), P(), P("tp", None), P("tp", None),
        ),
        out_specs=(P(("sp", "tp"), None), P("sp", "tp")),
        check_vma=False,
    )
```

```python
import functools

import jax
import jax.numpy as jnp
import numpy as np
from jax import lax
from jax.experimental import pallas as pl
from jax.experimental.pallas import tpu as pltpu
from jax.sharding import PartitionSpec as P

MESH = pl.DeviceIdType.MESH
BF = jnp.bfloat16
F32 = jnp.float32
ROPE_BASE = 500000.0
NORM_EPS = 1e-05
HEAD_KEEP = 0.8
MASKED = -1e30
LOG2E = float(np.log2(np.e))
LN2 = float(np.log(2.0))
NZ, NY, NX = 4, 4, 4
ROWS = 768
HD = 128
VD = 256
CH = 256
NCH = ROWS // CH
HF = CH // 2
PC = 32
BLK = 96


def vmem():
    return pl.BlockSpec(memory_space=pltpu.VMEM)


def hbm():
    return pl.BlockSpec(memory_space=pl.ANY)


def remote(src, dst, ssem, rsem, dev):
    return pltpu.make_async_remote_copy(
        src_ref=src, dst_ref=dst, send_sem=ssem, recv_sem=rsem, device_id=dev, device_id_type=MESH
    )


def scope(name):
    return jax.named_scope(name)


def greet(devs):
    barrier = pltpu.get_barrier_semaphore()
    for dev in devs:
        pl.semaphore_signal(barrier, inc=1, device_id=dev, device_id_type=MESH)
    pl.semaphore_wait(barrier, len(devs))


def layer_kernel(
    tok, gain, lam, hgain, taps, rc, rs, oc, os_, wq, wk, wv, wo, wi, ws, ap, cp,
    out, lse_ref,
    xbuf, sc, wbuf, apb, cpb, prod, outer, conv,
    qb, kvb, m_ref, l_ref, acc, lt, stats, dbuf, relay, fin,
    part, precv, xrelay, xfin,
    wsem, bsem, gss, grs, kss, krs, qss, qrs, tss, trs, dss, drs, pss, prs, xss, xrs,
):
    sp = lax.axis_index("sp")
    tp = lax.axis_index("tp")
    x, c = tp // 2, tp % 2
    z, y = sp // NY, sp % NY
    xr, xl, xo = lax.rem(x + 1, NX), lax.rem(x + 3, NX), lax.rem(x + 2, NX)
    yr, yl, yo = lax.rem(y + 1, NY), lax.rem(y + 3, NY), lax.rem(y + 2, NY)
    zr, zl, zo = lax.rem(z + 1, NZ), lax.rem(z + 3, NZ), lax.rem(z + 2, NZ)
    dxr, dxl, dm = (sp, xr * 2 + c), (sp, xl * 2 + c), (sp, x * 2 + (1 - c))
    dyr, dyl, dyo = (z * NY + yr, tp), (z * NY + yl, tp), (z * NY + yo, tp)
    dzr, dzl = (zr * NY + y, tp), (zl * NY + y, tp)
    dn, dp = (lax.rem(sp + 1, NZ * NY), tp), (lax.rem(sp + NZ * NY - 1, NZ * NY), tp)
    right, left, opp = xr * 2 + c, xl * 2 + c, xo * 2 + c

    weights = ((wk, wbuf.at[0]), (wv, wbuf.at[1]), (wq, wbuf.at[2]), (wi, wbuf.at[3]),
               (ws, wbuf.at[4]), (wo, wbuf.at[5]), (ap, apb), (cp, cpb))
    wcopies = [pltpu.make_async_copy(a, b, wsem.at[i]) for i, (a, b) in enumerate(weights)]
    for copy in wcopies:
        copy.start()
    for k in range(NCH):
        for t in range(2 * NX):
            xbuf[tp, k * CH + t * PC:k * CH + (t + 1) * PC, :] = tok[t * BLK + k * PC:t * BLK + (k + 1) * PC, :]
    with scope("greet"):
        greet([dxr, dxl, dm, dyr, dyl, dyo, dzr, dzl, dn, dp])
    sent = []

    def go(copy):
        copy.start()
        sent.append(copy)

    def rows_of(k, h=None):
        return pl.ds(k * CH, CH) if h is None else pl.ds(k * CH + h * HF, HF)

    def pass_on(k, kind, block, h, dev):
        ref = xbuf.at[block, rows_of(k, h)]
        return remote(ref, ref, gss.at[k, kind], grs.at[k, kind], dev)

    def send_own(k):
        go(pass_on(k, 0, tp, None, dxr))
        go(pass_on(k, 1, tp, None, dxl))
        go(pass_on(k, 2, tp, None, dm))

    def near(k):
        pass_on(k, 0, tp, None, dxr).wait_recv()
        go(pass_on(k, 3, left, 0, dxr))
        go(pass_on(k, 5, left, None, dm))
        pass_on(k, 1, tp, None, dxl).wait_recv()
        go(pass_on(k, 4, right, 1, dxl))
        go(pass_on(k, 6, right, None, dm))

    def far(k):
        pass_on(k, 3, left, 0, dxr).wait_recv()
        go(pass_on(k, 7, opp, 0, dm))
        pass_on(k, 4, right, 1, dxl).wait_recv()
        go(pass_on(k, 8, opp, 1, dm))

    def mates(k):
        pass_on(k, 2, tp, None, dm).wait_recv()
        pass_on(k, 5, left, None, dm).wait_recv()
        pass_on(k, 6, right, None, dm).wait_recv()
        pass_on(k, 7, opp, 0, dm).wait_recv()
        pass_on(k, 8, opp, 1, dm).wait_recv()

    def ring(buf, me, lf, rt, ss, rs_, d_r, d_l):
        def one(block, k, h, kind, dev):
            ref = buf.at[block, rows_of(k, h)]
            return remote(ref, ref, ss.at[k, kind], rs_.at[k, kind], dev)

        return [
            [one(me, k, 0, 0, d_r), one(me, k, 1, 1, d_r), one(me, k, 1, 2, d_l),
             one(me, k, 0, 3, d_l), one(lf, k, 0, 4, d_r), one(rt, k, 1, 5, d_l)]
            for k in range(NCH)
        ]

    kring = ring(kvb, z, zl, zr, kss, krs, dzr, dzl)
    qring = ring(qb, y, yl, yr, qss, qrs, dyr, dyl)

    def ring_send(copies):
        for i in (0, 2, 1, 3):
            go(copies[i])

    def ring_relay(copies):
        copies[0].wait_recv()
        go(copies[4])
        copies[2].wait_recv()
        go(copies[5])

    def ring_rest(rings):
        for copies in rings:
            copies[1].wait_recv()
            copies[3].wait_recv()

    def ring_far(rings):
        for copies in rings:
            copies[4].wait_recv()
            copies[5].wait_recv()

    co = oc[pl.ds(sp, 1), :]
    so = os_[pl.ds(sp, 1), :]

    def compute(k):
        rows = rows_of(k)
        square = jnp.zeros((CH, HD), F32)
        for b in range(2 * NX):
            xb = xbuf[b, rows, :].astype(F32)
            square += xb[:, :HD] * xb[:, :HD] + xb[:, HD:] * xb[:, HD:]
            sc[:, b * 256:(b + 1) * 256] = (xb * gain[:, b * 256:(b + 1) * 256]).astype(BF)
        total = jnp.sum(square, axis=1, keepdims=True)
        inv = lax.rsqrt(total / (2 * NX * 256) + NORM_EPS)
        c_r, s_r = rc[rows, :], rs[rows, :]
        cosine = co * c_r - so * s_r
        sine = so * c_r + co * s_r
        lane = lax.broadcasted_iota(jnp.int32, (CH, HD), 1)
        sine = jnp.where(lane < HD // 2, -sine, sine)

        def project(i):
            return inv * jnp.dot(sc[...], wbuf[i], preferred_element_type=F32)

        def turn(v):
            parts = []
            for j in range(2):
                t = v[:, j * HD:(j + 1) * HD]
                parts.append(t * cosine + pltpu.roll(t, HD // 2, 1) * sine)
            return jnp.concatenate(parts, axis=1)

        kvb[z, rows, 0:VD] = turn(project(0)).astype(BF)
        kvb[z, rows, VD:2 * VD] = project(1).astype(BF)
        qb[y, rows, :] = (turn(project(2)) * (LOG2E * HD ** -0.5)).astype(BF)
        ring_send(kring[k])
        ring_send(qring[k])
        pr = project(3) * project(4)
        og = project(5)
        for t in range(2 * NX):
            at = t * BLK + k * PC
            prod[8 + at:8 + at + PC, :] = pr[t * PC:(t + 1) * PC]
            outer[at:at + PC, :] = og[t * PC:(t + 1) * PC]

    def scores(qi, kj, rows, j):
        q = qb[qi, rows, j * HD:(j + 1) * HD]
        k = kvb[kj, :, j * HD:(j + 1) * HD]
        return lax.dot_general(q, k, (((1,), (1,)), ((), ())), preferred_element_type=F32)

    def absorb(qi, kj, rows, j, s):
        before = m_ref[j, qi, rows, :]
        now = jnp.maximum(before, jnp.max(s, axis=1, keepdims=True))
        fade = jnp.exp2(before - now)
        p = jnp.exp2(s - jnp.concatenate([now] * (ROWS // HD), axis=1))
        total = l_ref[j, qi, rows, :] * fade
        for i in range(ROWS // HD):
            total = total + p[:, i * HD:(i + 1) * HD]
        l_ref[j, qi, rows, :] = total
        m_ref[j, qi, rows, :] = now
        acc[j, qi, rows, :] = acc[j, qi, rows, :] * jnp.concatenate([fade] * 2, axis=1) + jnp.dot(
            p.astype(BF), kvb[kj, :, VD:2 * VD], preferred_element_type=F32
        )

    def attend(qi, kj, rows, mask=None):
        ss = [scores(qi, kj, rows, j) for j in range(2)]
        for j in range(2):
            s = ss[j] if mask is None else jnp.where(mask, ss[j], MASKED)
            absorb(qi, kj, rows, j, s)

    def place(p):
        return ((p >> 5) & 7) * BLK + (p >> 8) * PC + (p & 31)

    def own_pair():
        row = place(lax.broadcasted_iota(jnp.int32, (ROWS, HD), 0))
        row = jnp.concatenate([row] * (ROWS // HD), axis=1)
        col = place(lax.broadcasted_iota(jnp.int32, (1, ROWS), 1))
        attend(y, z, pl.ds(0, ROWS), col <= row)

    def start():
        m_ref[...] = jnp.full(m_ref.shape, MASKED, F32)
        l_ref[...] = jnp.zeros(l_ref.shape, F32)
        acc[...] = jnp.zeros(acc.shape, F32)

    send_own(0)
    send_own(1)
    start()
    with scope("near0"):
        near(0)
    with scope("near1"):
        near(1)
    send_own(2)
    with scope("far0"):
        far(0)
    with scope("mates0"):
        mates(0)
        for copy in wcopies:
            copy.wait()
    with scope("comp0"):
        compute(0)
    with scope("near2"):
        near(2)
    with scope("far1"):
        far(1)
        mates(1)
    with scope("comp1"):
        compute(1)
    with scope("far2"):
        far(2)
        mates(2)
    with scope("qrel0"):
        ring_relay(qring[0])
    with scope("comp2"):
        compute(2)
    border = remote(prod.at[pl.ds(ROWS, 8)], prod.at[pl.ds(0, 8)], bsem.at[0], bsem.at[1], dn)
    go(border)
    with scope("rel0"):
        ring_relay(kring[0])
        ring_relay(qring[1])
    with scope("own"):
        own_pair()
    with scope("rel1"):
        ring_relay(kring[1])
        ring_relay(qring[2])
    with scope("conv"):
        border.wait_recv()

        @pl.when(sp == 0)
        def _():
            prod[0:8, :] = jnp.zeros((8, 256), F32)

        tv = taps[...].astype(F32)
        smoothed = (
            tv[0:1] * prod[6:6 + ROWS, :] + tv[1:2] * prod[7:7 + ROWS, :] + tv[2:3] * prod[8:8 + ROWS, :]
        )
        conv[...] = (outer[...] * smoothed).astype(BF)
    with scope("qrest"):
        ring_rest(qring)

    def step(i, _):
        @pl.when(i == 2)
        def _():
            with scope("qfar"):
                ring_far(qring)
            with scope("rel2"):
                ring_relay2()

        @pl.when(i == 3)
        def _():
            with scope("krest"):
                ring_rest(kring)

        mine = i < 3
        first = i < 7
        turn_ = jnp.where(i == 0, 1, jnp.where(i == 1, 3, 2))
        qi = jnp.where(mine, lax.rem(y + turn_, NY), lax.rem(i + 1, NY))
        kj = jnp.where(mine, z, jnp.where(first, zl, zr))
        need = (mine & (qi > y)) | (~mine & first & (z >= 1)) | (~first & (z == 3))

        @pl.when(need)
        def _():
            with scope("item"):
                attend(qi, kj, pl.ds(0, ROWS))

        return 0

    def ring_relay2():
        copies = kring[2]
        copies[0].wait_recv()
        copies[4].start()
        copies[2].wait_recv()
        copies[5].start()

    lax.fori_loop(0, 11, step, 0)
    sent.append(kring[2][4])
    sent.append(kring[2][5])
    with scope("kfar"):
        ring_far(kring)

    lam_v = lam[...]

    def last_keys(k):
        @pl.when(z >= 2)
        def _():
            ss = [[scores(qi, zo, rows_of(k), j) for qi in range(NY)] for j in range(2)]
            for j in range(2):
                for qi in range(NY):
                    absorb(qi, zo, rows_of(k), j, ss[j][qi])

    def stat_copies(k):
        ref = stats.at[y, k]
        return [
            remote(ref, ref, tss.at[k, i], trs.at[k, i], dev) for i, dev in enumerate((dyr, dyl, dyo))
        ]

    def send_stats(k):
        rows = rows_of(k)
        lane = lax.broadcasted_iota(jnp.int32, (CH, HD), 1)
        table = jnp.full((CH, HD), MASKED, F32)
        for qi in range(NY):
            for j in range(2):
                total = jnp.sum(l_ref[j, qi, rows, :], axis=1, keepdims=True)
                lse = m_ref[j, qi, rows, :] + jnp.log2(jnp.maximum(total, 1e-37))
                table = jnp.where(lane == 2 * qi + j, lse, table)
        stats[y, k] = jnp.transpose(table)[0:8, :]
        for copy in stat_copies(k):
            go(copy)

    def pick(rows, qi, j):
        lanes = lax.broadcasted_iota(jnp.int32, (CH, HD), 1)
        return jnp.sum(jnp.where(lanes == 2 * qi + j, lt[rows, :], 0.0), axis=1, keepdims=True)

    def share(rows, qi):
        outs = []
        for j in range(2):
            f = jnp.exp2(m_ref[j, qi, rows, :] - pick(rows, qi, j))
            outs.append(acc[j, qi, rows, :] * jnp.concatenate([f] * 2, axis=1))
        return outs[0] - lam_v * outs[1]

    def scatter(k):
        h0, h1 = rows_of(k, 0), rows_of(k, 1)
        at = pl.ds(k * HF, HF)
        pairs = [
            (dbuf.at[yo, h0], relay.at[0, at], dyr),
            (dbuf.at[yo, h1], relay.at[1, at], dyl),
            (dbuf.at[yr, h1], fin.at[0, h1], dyr),
            (dbuf.at[yl, h0], fin.at[1, h0], dyl),
            (dbuf.at[yr, h0], fin.at[0, h0], dyr),
            (dbuf.at[yl, h1], fin.at[1, h1], dyl),
        ]
        return [remote(a, b, dss.at[k, i], drs.at[k, i], d) for i, (a, b, d) in enumerate(pairs)]

    def send_shares(k):
        rows = rows_of(k)
        for copy in stat_copies(k):
            copy.wait_recv()
        parts = [stats[i, k] for i in range(NY)]
        peak = jnp.maximum(jnp.maximum(parts[0], parts[1]), jnp.maximum(parts[2], parts[3]))
        whole = peak + jnp.log2(sum(jnp.exp2(p - peak) for p in parts))
        lt[rows, :] = jnp.transpose(jnp.concatenate([whole, jnp.zeros((HD - 8, CH), F32)], axis=0))

        def one(i, _):
            qi = lax.rem(y + jnp.where(i == 0, 2, jnp.where(i == 1, 1, 3)), NY)
            dbuf[qi, rows, :] = share(rows, qi).astype(BF)
            return 0

        lax.fori_loop(0, NY - 1, one, 0)
        for copy in scatter(k)[:4]:
            go(copy)

    def join_shares(k):
        copies = scatter(k)
        h0, h1 = rows_of(k, 0), rows_of(k, 1)
        at = pl.ds(k * HF, HF)
        copies[0].wait_recv()
        dbuf[yr, h0, :] = (dbuf[yr, h0, :].astype(F32) + relay[0, at, :].astype(F32)).astype(BF)
        go(copies[4])
        copies[1].wait_recv()
        dbuf[yl, h1, :] = (dbuf[yl, h1, :].astype(F32) + relay[1, at, :].astype(F32)).astype(BF)
        go(copies[5])

    def mate_copy(k):
        return remote(part.at[k, 1 - c], precv.at[k], pss.at[k], prs.at[k], dm)

    def merge(k):
        rows = rows_of(k)
        for copy in scatter(k)[2:]:
            copy.wait_recv()
        d = share(rows, y) + fin[0, rows, :].astype(F32) + fin[1, rows, :].astype(F32)
        back = lax.rsqrt(jnp.mean(d * d, axis=1, keepdims=True) + NORM_EPS)
        att = (d * back * hgain[...] * HEAD_KEEP).astype(BF)
        ls = [pick(rows, y, j) * LN2 for j in range(2)]
        pieces = [slice(t * BLK + k * PC, t * BLK + (k + 1) * PC) for t in range(2 * NX)]
        for t in range(2 * NX):
            for j in range(2):
                lse_ref[pieces[t], j:j + 1] = ls[j][t * PC:(t + 1) * PC]
        con = jnp.concatenate([conv[pieces[t], :] for t in range(2 * NX)], axis=0)
        cols = 512
        for n in range(2048 // cols):
            cs = slice(n * cols, (n + 1) * cols)
            p = jnp.dot(att, apb[:, cs], preferred_element_type=F32) + jnp.dot(
                con, cpb[:, cs], preferred_element_type=F32
            )
            p = p.astype(BF)
            for t in range(2 * NX):
                part[k, t % 2, t // 2, :, cs] = p[t * PC:(t + 1) * PC]
        go(mate_copy(k))

    g0, g1 = pl.ds(0, PC // 2), pl.ds(PC // 2, PC // 2)

    def spread(k):
        pairs = [
            (part.at[k, c, xo, g0], xrelay.at[k, 0], dxr),
            (part.at[k, c, xo, g1], xrelay.at[k, 1], dxl),
            (part.at[k, c, xr, g1], xfin.at[k, 0, g1], dxr),
            (part.at[k, c, xl, g0], xfin.at[k, 1, g0], dxl),
            (part.at[k, c, xr, g0], xfin.at[k, 0, g0], dxr),
            (part.at[k, c, xl, g1], xfin.at[k, 1, g1], dxl),
        ]
        return [remote(a, b, xss.at[k, i], xrs.at[k, i], d) for i, (a, b, d) in enumerate(pairs)]

    def add_mate(k, xx, g, extra=None):
        t = part[k, c, xx, g, :].astype(F32) + precv[k, xx, g, :].astype(F32)
        if extra is not None:
            t = t + extra.astype(F32)
        part[k, c, xx, g, :] = t.astype(BF)

    def send_sums(k):
        copies = spread(k)
        mate_copy(k).wait_recv()
        add_mate(k, xo, pl.ds(0, PC))
        add_mate(k, xr, g1)
        add_mate(k, xl, g0)
        for copy in copies[:4]:
            go(copy)

    def join_sums(k):
        copies = spread(k)
        copies[0].wait_recv()
        add_mate(k, xr, g0, xrelay[k, 0])
        go(copies[4])
        copies[1].wait_recv()
        add_mate(k, xl, g1, xrelay[k, 1])
        go(copies[5])

    def finish(k):
        for copy in spread(k)[2:]:
            copy.wait_recv()
        total = part[k, c, x].astype(F32) + precv[k, x].astype(F32)
        total = total + xfin[k, 0].astype(F32) + xfin[k, 1].astype(F32)
        out[k * PC:(k + 1) * PC, :] = total.astype(BF)

    plan = (
        (last_keys, 0), (send_stats, 0), (last_keys, 1), (send_stats, 1), (send_shares, 0),
        (last_keys, 2), (send_stats, 2), (send_shares, 1), (join_shares, 0), (send_shares, 2),
        (join_shares, 1), (merge, 0), (join_shares, 2), (send_sums, 0), (merge, 1), (join_sums, 0),
        (send_sums, 1), (merge, 2), (join_sums, 1), (send_sums, 2), (finish, 0), (join_sums, 2),
        (finish, 1), (finish, 2),
    )
    for f, k in plan:
        with scope(f"{f.__name__}{k}"):
            f(k)
    with scope("drain"):
        for copy in sent:
            copy.wait_send()


def tables():
    inverse = ROPE_BASE ** (-np.arange(HD // 2, dtype=np.float64) * 2.0 / HD)
    inverse = inverse.astype(np.float32).astype(np.float64)
    inverse = np.concatenate([inverse, inverse])
    place = np.arange(ROWS).reshape(2 * NX, NCH, PC).transpose(1, 0, 2).reshape(-1)
    local = place[:, None] * inverse[None, :]
    offset = (np.arange(NZ * NY) * ROWS)[:, None] * inverse[None, :]
    return [f(a).astype(np.float32) for a in (local, offset) for f in (np.cos, np.sin)]


DMA = pltpu.SemaphoreType.DMA


def per_device(
    tokens, norm_gain, w_query, w_key, w_value, w_outer, w_inner, w_signal,
    conv_taps, lambdas, head_gain, attend_proj, convolve_proj,
):
    rc, rs, oc, os_ = tables()
    v = pltpu.VMEM
    mixed, lse = pl.pallas_call(
        layer_kernel,
        out_shape=(
            jax.ShapeDtypeStruct((BLK, 2048), BF),
            jax.ShapeDtypeStruct((ROWS, 2), F32),
        ),
        in_specs=[vmem()] * 9 + [hbm()] * 8,
        out_specs=(vmem(), vmem()),
        scratch_shapes=[
            v((2 * NX, ROWS, 256), BF), v((CH, 2048), BF), v((6, 2048, 256), BF),
            v((256, 2048), BF), v((256, 2048), BF),
            v((ROWS + 8, 256), F32), v((ROWS, 256), F32), v((ROWS, 256), BF),
            v((NY, ROWS, VD), BF), v((NZ, ROWS, 2 * VD), BF),
            v((2, NY, ROWS, HD), F32), v((2, NY, ROWS, HD), F32), v((2, NY, ROWS, VD), F32),
            v((ROWS, HD), F32), v((NY, NCH, 8, CH), F32), v((NY, ROWS, VD), BF),
            v((2, NCH * HF, VD), BF), v((2, ROWS, VD), BF),
            v((NCH, 2, NX, PC, 2048), BF), v((NCH, NX, PC, 2048), BF),
            v((NCH, 2, PC // 2, 2048), BF), v((NCH, 2, PC, 2048), BF),
            DMA((8,)), DMA((2,)), DMA((NCH, 9)), DMA((NCH, 9)),
            DMA((NCH, 6)), DMA((NCH, 6)), DMA((NCH, 6)), DMA((NCH, 6)),
            DMA((NCH, 3)), DMA((NCH, 3)), DMA((NCH, 6)), DMA((NCH, 6)),
            DMA((NCH,)), DMA((NCH,)), DMA((NCH, 6)), DMA((NCH, 6)),
        ],
        compiler_params=pltpu.CompilerParams(
            collective_id=1, has_side_effects=True, vmem_limit_bytes=62 * 2 ** 20
        ),
        name="layer",
    )(
        tokens, norm_gain.reshape(1, -1), lambdas.reshape(1, 1), head_gain.reshape(1, -1), conv_taps,
        rc, rs, oc, os_, w_query, w_key, w_value, w_outer, w_inner, w_signal, attend_proj, convolve_proj,
    )
    return mixed, lse


def solution(mesh):
    return jax.shard_map(
        per_device,
        mesh=mesh,
        in_specs=(
            P("sp", "tp"), P(), P(None, "tp"), P(None, "tp"), P(None, "tp"), P(None, "tp"),
            P(None, "tp"), P(None, "tp"), P(None, "tp"), P("tp"), P(), P("tp", None), P("tp", None),
        ),
        out_specs=(P(("sp", "tp"), None), P("sp", "tp")),
        check_vma=False,
    )
```

```python
import functools

import jax
import jax.numpy as jnp
import numpy as np
from jax import lax
from jax.experimental import pallas as pl
from jax.experimental.pallas import tpu as pltpu
from jax.sharding import PartitionSpec as P

MESH = pl.DeviceIdType.MESH
BF = jnp.bfloat16
F32 = jnp.float32
ROPE_BASE = 500000.0
NORM_EPS = 1e-05
HEAD_KEEP = 0.8
MASKED = -1e30
LOG2E = float(np.log2(np.e))
LN2 = float(np.log(2.0))
NZ, NY, NX = 4, 4, 4
ROWS = 768
HD = 128
VD = 256
CH = 256
NCH = ROWS // CH
HF = CH // 2
PC = 32
BLK = 96


def vmem():
    return pl.BlockSpec(memory_space=pltpu.VMEM)


def hbm():
    return pl.BlockSpec(memory_space=pl.ANY)


def remote(src, dst, ssem, rsem, dev):
    return pltpu.make_async_remote_copy(
        src_ref=src, dst_ref=dst, send_sem=ssem, recv_sem=rsem, device_id=dev, device_id_type=MESH
    )


def scope(name):
    return jax.named_scope(name)


def greet(devs):
    barrier = pltpu.get_barrier_semaphore()
    for dev in devs:
        pl.semaphore_signal(barrier, inc=1, device_id=dev, device_id_type=MESH)
    pl.semaphore_wait(barrier, len(devs))


def layer_kernel(
    gain, lam, hgain, taps, oc, os_, tok, rch, rsh, wq, wk, wv, wo, wi, ws, ap, cp,
    out, lse_ref,
    xbuf, gcol, rc, rs, wbuf, apb, cpb, prod, outer, conv, lnat, obuf,
    qb, kvb, m_ref, l_ref, acc, lt, stats, dbuf, relay, fin,
    part, precv, xrelay, xfin,
    wsem, tsem, osem, bsem, gss, grs, kss, krs, qss, qrs, tss, trs, dss, drs, pss, prs, xss, xrs,
):
    sp = lax.axis_index("sp")
    tp = lax.axis_index("tp")
    x, c = tp // 2, tp % 2
    z, y = sp // NY, sp % NY
    xr, xl, xo = lax.rem(x + 1, NX), lax.rem(x + 3, NX), lax.rem(x + 2, NX)
    yr, yl, yo = lax.rem(y + 1, NY), lax.rem(y + 3, NY), lax.rem(y + 2, NY)
    zr, zl, zo = lax.rem(z + 1, NZ), lax.rem(z + 3, NZ), lax.rem(z + 2, NZ)
    dxr, dxl, dm = (sp, xr * 2 + c), (sp, xl * 2 + c), (sp, x * 2 + (1 - c))
    dyr, dyl, dyo = (z * NY + yr, tp), (z * NY + yl, tp), (z * NY + yo, tp)
    dzr, dzl = (zr * NY + y, tp), (zl * NY + y, tp)
    dn, dp = (lax.rem(sp + 1, NZ * NY), tp), (lax.rem(sp + NZ * NY - 1, NZ * NY), tp)
    right, left, opp = xr * 2 + c, xl * 2 + c, xo * 2 + c

    tcopies = [
        pltpu.make_async_copy(tok.at[:, pl.ds(k * PC, PC), :], xbuf.at[tp, k], tsem.at[k])
        for k in range(NCH)
    ]
    for copy in tcopies:
        copy.start()
    weights = ((wk, wbuf.at[0]), (wv, wbuf.at[1]), (wq, wbuf.at[2]), (wi, wbuf.at[3]),
               (ws, wbuf.at[4]), (wo, wbuf.at[5]), (rch, rc), (rsh, rs), (ap, apb), (cp, cpb))
    wcopies = [pltpu.make_async_copy(a, b, wsem.at[i]) for i, (a, b) in enumerate(weights)]
    for copy in wcopies:
        copy.start()
    with scope("greet"):
        greet([dxr, dxl, dm, dyr, dyl, dyo, dzr, dzl, dn, dp])
    sent = []

    def go(copy):
        copy.start()
        sent.append(copy)

    def rows_of(k, h=None):
        return pl.ds(k * CH, CH) if h is None else pl.ds(k * CH + h * HF, HF)

    def pass_on(k, kind, block, h, dev):
        ref = xbuf.at[block, k] if h is None else xbuf.at[block, k, pl.ds(h * NX, NX)]
        return remote(ref, ref, gss.at[k, kind], grs.at[k, kind], dev)

    def send_own(k):
        tcopies[k].wait()
        go(pass_on(k, 0, tp, None, dxr))
        go(pass_on(k, 1, tp, None, dxl))
        go(pass_on(k, 2, tp, None, dm))

    def near(k):
        pass_on(k, 0, tp, None, dxr).wait_recv()
        go(pass_on(k, 3, left, 0, dxr))
        go(pass_on(k, 5, left, None, dm))
        pass_on(k, 1, tp, None, dxl).wait_recv()
        go(pass_on(k, 4, right, 1, dxl))
        go(pass_on(k, 6, right, None, dm))

    def far(k):
        pass_on(k, 3, left, 0, dxr).wait_recv()
        go(pass_on(k, 7, opp, 0, dm))
        pass_on(k, 4, right, 1, dxl).wait_recv()
        go(pass_on(k, 8, opp, 1, dm))

    def mates(k):
        pass_on(k, 2, tp, None, dm).wait_recv()
        pass_on(k, 5, left, None, dm).wait_recv()
        pass_on(k, 6, right, None, dm).wait_recv()
        pass_on(k, 7, opp, 0, dm).wait_recv()
        pass_on(k, 8, opp, 1, dm).wait_recv()

    def ring(buf, me, lf, rt, ss, rs_, d_r, d_l):
        def one(block, k, h, kind, dev):
            ref = buf.at[block, rows_of(k, h)]
            return remote(ref, ref, ss.at[k, kind], rs_.at[k, kind], dev)

        return [
            [one(me, k, 0, 0, d_r), one(me, k, 1, 1, d_r), one(me, k, 1, 2, d_l),
             one(me, k, 0, 3, d_l), one(lf, k, 0, 4, d_r), one(rt, k, 1, 5, d_l)]
            for k in range(NCH)
        ]

    kring = ring(kvb, z, zl, zr, kss, krs, dzr, dzl)
    qring = ring(qb, y, yl, yr, qss, qrs, dyr, dyl)

    def ring_send(copies):
        for i in (0, 2, 1, 3):
            go(copies[i])

    def ring_relay(copies):
        copies[0].wait_recv()
        go(copies[4])
        copies[2].wait_recv()
        go(copies[5])

    def ring_rest(rings):
        for copies in rings:
            copies[1].wait_recv()
            copies[3].wait_recv()

    def ring_right(rings):
        for copies in rings:
            copies[3].wait_recv()

    def ring_far(rings):
        for copies in rings:
            copies[4].wait_recv()
            copies[5].wait_recv()

    co = oc[pl.ds(sp, 1), :]
    so = os_[pl.ds(sp, 1), :]

    def compute(k):
        rows = rows_of(k)
        square = jnp.zeros((CH, HD), F32)
        blocks = [xbuf[b, k].reshape(CH, 256) for b in range(2 * NX)]
        for xb in blocks:
            xf = xb.astype(F32)
            square += xf[:, :HD] * xf[:, :HD] + xf[:, HD:] * xf[:, HD:]
        wide = jnp.concatenate(blocks, axis=1)
        total = jnp.sum(square, axis=1, keepdims=True)
        inv = lax.rsqrt(total / (2 * NX * 256) + NORM_EPS)
        c_r, s_r = rc[rows, :], rs[rows, :]
        cosine = co * c_r - so * s_r
        sine = so * c_r + co * s_r
        lane = lax.broadcasted_iota(jnp.int32, (CH, HD), 1)
        sine = jnp.where(lane < HD // 2, -sine, sine)

        def project(i):
            return inv * jnp.dot(wide, wbuf[i], preferred_element_type=F32)

        def turn(v):
            parts = []
            for j in range(2):
                t = v[:, j * HD:(j + 1) * HD]
                parts.append(t * cosine + pltpu.roll(t, HD // 2, 1) * sine)
            return jnp.concatenate(parts, axis=1)

        kvb[z, rows, 0:VD] = turn(project(0)).astype(BF)
        kvb[z, rows, VD:2 * VD] = project(1).astype(BF)
        qb[y, rows, :] = (turn(project(2)) * (LOG2E * HD ** -0.5)).astype(BF)
        ring_send(kring[k])
        ring_send(qring[k])
        pr = project(3) * project(4)
        og = project(5)
        for t in range(2 * NX):
            at = t * BLK + k * PC
            prod[8 + at:8 + at + PC, :] = pr[t * PC:(t + 1) * PC]
            outer[at:at + PC, :] = og[t * PC:(t + 1) * PC]

    def scores(qi, kj, rows, j):
        q = qb[qi, rows, j * HD:(j + 1) * HD]
        k = kvb[kj, :, j * HD:(j + 1) * HD]
        return lax.dot_general(q, k, (((1,), (1,)), ((), ())), preferred_element_type=F32)

    def absorb(qi, kj, rows, j, s):
        before = m_ref[j, qi, rows, :]
        now = jnp.maximum(before, jnp.max(s, axis=1, keepdims=True))
        fade = jnp.exp2(before - now)
        p = jnp.exp2(s - jnp.concatenate([now] * (ROWS // HD), axis=1))
        total = l_ref[j, qi, rows, :] * fade
        for i in range(ROWS // HD):
            total = total + p[:, i * HD:(i + 1) * HD]
        l_ref[j, qi, rows, :] = total
        m_ref[j, qi, rows, :] = now
        acc[j, qi, rows, :] = acc[j, qi, rows, :] * jnp.concatenate([fade] * 2, axis=1) + jnp.dot(
            p.astype(BF), kvb[kj, :, VD:2 * VD], preferred_element_type=F32
        )

    def attend(qi, kj, rows, mask=None):
        ss = [scores(qi, kj, rows, j) for j in range(2)]
        for j in range(2):
            s = ss[j] if mask is None else jnp.where(mask, ss[j], MASKED)
            absorb(qi, kj, rows, j, s)

    def place(p):
        return ((p >> 5) & 7) * BLK + (p >> 8) * PC + (p & 31)

    def own_pair():
        row = place(lax.broadcasted_iota(jnp.int32, (ROWS, HD), 0))
        row = jnp.concatenate([row] * (ROWS // HD), axis=1)
        col = place(lax.broadcasted_iota(jnp.int32, (1, ROWS), 1))
        attend(y, z, pl.ds(0, ROWS), col <= row)

    def scale_weights():
        g = jnp.concatenate([gain[...], jnp.zeros((HD - 16, HD), F32)], axis=0)
        g = jnp.transpose(g)
        for b in range(16):
            gcol[b * HD:(b + 1) * HD, :] = jnp.broadcast_to(g[:, b:b + 1], (HD, HD))

        def one(i, _):
            for b in range(8):
                rows = slice(b * 256, (b + 1) * 256)
                col = gcol[rows, :]
                w = wbuf[i, rows, :].astype(F32)
                wbuf[i, rows, :] = (w * jnp.concatenate([col, col], axis=1)).astype(BF)
            return 0

        lax.fori_loop(0, 6, one, 0)

    def start():
        m_ref[...] = jnp.full(m_ref.shape, MASKED, F32)
        l_ref[...] = jnp.zeros(l_ref.shape, F32)
        acc[...] = jnp.zeros(acc.shape, F32)

    send_own(0)
    send_own(1)
    with scope("init"):
        start()
        for copy in wcopies:
            copy.wait()
    with scope("scale"):
        scale_weights()
    with scope("near0"):
        near(0)
    with scope("near1"):
        near(1)
    send_own(2)
    with scope("far0"):
        far(0)
    with scope("mates0"):
        mates(0)
    with scope("comp0"):
        compute(0)
    with scope("near2"):
        near(2)
    with scope("far1"):
        far(1)
        mates(1)
    with scope("comp1"):
        compute(1)
    with scope("far2"):
        far(2)
        mates(2)
    with scope("qrel0"):
        ring_relay(qring[0])
    with scope("comp2"):
        compute(2)
    border = remote(prod.at[pl.ds(ROWS, 8)], prod.at[pl.ds(0, 8)], bsem.at[0], bsem.at[1], dn)
    go(border)
    with scope("rel0"):
        ring_relay(kring[0])
        ring_relay(qring[1])
    with scope("own"):
        own_pair()
    with scope("rel1"):
        ring_relay(kring[1])
        ring_relay(qring[2])
    with scope("conv"):
        border.wait_recv()

        @pl.when(sp == 0)
        def _():
            prod[0:8, :] = jnp.zeros((8, 256), F32)

        tv = taps[...].astype(F32)
        smoothed = (
            tv[0:1] * prod[6:6 + ROWS, :] + tv[1:2] * prod[7:7 + ROWS, :] + tv[2:3] * prod[8:8 + ROWS, :]
        )
        conv[...] = (outer[...] * smoothed).astype(BF)
    with scope("qrest"):
        ring_rest(qring)

    def step(i, _):
        @pl.when(i == 2)
        def _():
            with scope("qfar"):
                ring_far(qring)
            with scope("rel2"):
                ring_relay2()

        @pl.when(i == 3)
        def _():
            with scope("krest"):
                for copies in kring:
                    copies[1].wait_recv()

        mine = i < 3
        turn_ = jnp.where(i == 0, 1, jnp.where(i == 1, 3, 2))
        qi = jnp.where(mine, lax.rem(y + turn_, NY), lax.rem(i + 1, NY))
        kj = jnp.where(mine, z, zl)
        need = (mine & (qi > y)) | (~mine & (z >= 1))

        @pl.when(need)
        def _():
            with scope("item"):
                attend(qi, kj, pl.ds(0, ROWS))

        return 0

    def ring_relay2():
        copies = kring[2]
        copies[0].wait_recv()
        copies[4].start()
        copies[2].wait_recv()
        copies[5].start()

    lax.fori_loop(0, 7, step, 0)
    sent.append(kring[2][4])
    sent.append(kring[2][5])
    lam_v = lam[0]

    def last_keys(k, between):
        def body(i, _):
            right_turn = i == 0
            if k == 0:
                @pl.when(right_turn)
                def _():
                    with scope("kright"):
                        ring_right(kring)

                @pl.when(i == 1)
                def _():
                    with scope("kfar"):
                        ring_far(kring)

            kj = jnp.where(right_turn, zr, zo)

            @pl.when((z == 3) | ((i == 1) & (z == 2)))
            def _():
                with scope("tiles"):
                    ss = [[scores(qi, kj, rows_of(k), j) for qi in range(NY)] for j in range(2)]
                    for j in range(2):
                        for qi in range(NY):
                            absorb(qi, kj, rows_of(k), j, ss[j][qi])

            if between:
                @pl.when(right_turn)
                def _():
                    for f, kk in between:
                        with scope(f"{f.__name__}{kk}"):
                            f(kk)

            return 0

        lax.fori_loop(0, 2, body, 0)

    def stat_copies(k):
        ref = stats.at[y, k]
        return [
            remote(ref, ref, tss.at[k, i], trs.at[k, i], dev) for i, dev in enumerate((dyr, dyl, dyo))
        ]

    def send_stats(k):
        rows = rows_of(k)
        lane = lax.broadcasted_iota(jnp.int32, (CH, HD), 1)
        table = jnp.full((CH, HD), MASKED, F32)
        for qi in range(NY):
            for j in range(2):
                total = jnp.sum(l_ref[j, qi, rows, :], axis=1, keepdims=True)
                lse = m_ref[j, qi, rows, :] + jnp.log2(jnp.maximum(total, 1e-37))
                table = jnp.where(lane == 2 * qi + j, lse, table)
        stats[y, k] = jnp.transpose(table)[0:8, :]
        for copy in stat_copies(k):
            copy.start()

    def pick(rows, qi, j):
        lanes = lax.broadcasted_iota(jnp.int32, (CH, HD), 1)
        return jnp.sum(jnp.where(lanes == 2 * qi + j, lt[rows, :], 0.0), axis=1, keepdims=True)

    def share(rows, qi):
        outs = []
        for j in range(2):
            f = jnp.exp2(m_ref[j, qi, rows, :] - pick(rows, qi, j))
            outs.append(acc[j, qi, rows, :] * jnp.concatenate([f] * 2, axis=1))
        return outs[0] - lam_v * outs[1]

    def scatter(k):
        h0, h1 = rows_of(k, 0), rows_of(k, 1)
        at = pl.ds(k * HF, HF)
        pairs = [
            (dbuf.at[yo, h0], relay.at[0, at], dyr),
            (dbuf.at[yo, h1], relay.at[1, at], dyl),
            (dbuf.at[yr, h1], fin.at[0, h1], dyr),
            (dbuf.at[yl, h0], fin.at[1, h0], dyl),
            (dbuf.at[yr, h0], fin.at[0, h0], dyr),
            (dbuf.at[yl, h1], fin.at[1, h1], dyl),
        ]
        return [remote(a, b, dss.at[k, i], drs.at[k, i], d) for i, (a, b, d) in enumerate(pairs)]

    def send_shares(k):
        rows = rows_of(k)
        for copy in stat_copies(k):
            copy.wait_recv()
        parts = [stats[i, k] for i in range(NY)]
        peak = jnp.maximum(jnp.maximum(parts[0], parts[1]), jnp.maximum(parts[2], parts[3]))
        whole = peak + jnp.log2(sum(jnp.exp2(p - peak) for p in parts))
        lt[rows, :] = jnp.transpose(jnp.concatenate([whole, jnp.zeros((HD - 8, CH), F32)], axis=0))

        def one(i, _):
            qi = lax.rem(y + jnp.where(i == 0, 2, jnp.where(i == 1, 1, 3)), NY)
            dbuf[qi, rows, :] = share(rows, qi).astype(BF)
            return 0

        lax.fori_loop(0, NY - 1, one, 0)
        for copy in scatter(k)[:4]:
            copy.start()

    def join_shares(k):
        copies = scatter(k)
        h0, h1 = rows_of(k, 0), rows_of(k, 1)
        at = pl.ds(k * HF, HF)
        copies[0].wait_recv()
        dbuf[yr, h0, :] = (dbuf[yr, h0, :].astype(F32) + relay[0, at, :].astype(F32)).astype(BF)
        copies[4].start()
        copies[1].wait_recv()
        dbuf[yl, h1, :] = (dbuf[yl, h1, :].astype(F32) + relay[1, at, :].astype(F32)).astype(BF)
        copies[5].start()

    def mate_copy(k):
        return remote(part.at[k, 1 - c], precv.at[k], pss.at[k], prs.at[k], dm)

    def merge(k):
        rows = rows_of(k)
        for copy in scatter(k)[2:]:
            copy.wait_recv()
        d = share(rows, y) + fin[0, rows, :].astype(F32) + fin[1, rows, :].astype(F32)
        back = lax.rsqrt(jnp.mean(d * d, axis=1, keepdims=True) + NORM_EPS)
        att = (d * back * hgain[...] * HEAD_KEEP).astype(BF)
        pieces = [slice(t * BLK + k * PC, t * BLK + (k + 1) * PC) for t in range(2 * NX)]
        for t in range(2 * NX):
            lnat[pieces[t], :] = lt[k * CH + t * PC:k * CH + (t + 1) * PC, :]
        con = jnp.concatenate([conv[pieces[t], :] for t in range(2 * NX)], axis=0)
        cols = 512
        for n in range(2048 // cols):
            cs = slice(n * cols, (n + 1) * cols)
            p = jnp.dot(att, apb[:, cs], preferred_element_type=F32) + jnp.dot(
                con, cpb[:, cs], preferred_element_type=F32
            )
            p = p.astype(BF)
            for t in range(2 * NX):
                part[k, t % 2, t // 2, :, cs] = p[t * PC:(t + 1) * PC]
        mate_copy(k).start()

    g0, g1 = pl.ds(0, PC // 2), pl.ds(PC // 2, PC // 2)

    def spread(k):
        pairs = [
            (part.at[k, c, xo, g0], xrelay.at[k, 0], dxr),
            (part.at[k, c, xo, g1], xrelay.at[k, 1], dxl),
            (part.at[k, c, xr, g1], xfin.at[k, 0, g1], dxr),
            (part.at[k, c, xl, g0], xfin.at[k, 1, g0], dxl),
            (part.at[k, c, xr, g0], xfin.at[k, 0, g0], dxr),
            (part.at[k, c, xl, g1], xfin.at[k, 1, g1], dxl),
        ]
        return [remote(a, b, xss.at[k, i], xrs.at[k, i], d) for i, (a, b, d) in enumerate(pairs)]

    def add_mate(k, xx, g, extra=None):
        t = part[k, c, xx, g, :].astype(F32) + precv[k, xx, g, :].astype(F32)
        if extra is not None:
            t = t + extra.astype(F32)
        part[k, c, xx, g, :] = t.astype(BF)

    def send_sums(k):
        copies = spread(k)
        mate_copy(k).wait_recv()
        add_mate(k, xo, pl.ds(0, PC))
        add_mate(k, xr, g1)
        add_mate(k, xl, g0)
        for copy in copies[:4]:
            copy.start()

    def join_sums(k):
        copies = spread(k)
        copies[0].wait_recv()
        add_mate(k, xr, g0, xrelay[k, 0])
        copies[4].start()
        copies[1].wait_recv()
        add_mate(k, xl, g1, xrelay[k, 1])
        copies[5].start()

    def finish(k):
        for copy in spread(k)[2:]:
            copy.wait_recv()
        total = part[k, c, x].astype(F32) + precv[k, x].astype(F32)
        total = total + xfin[k, 0].astype(F32) + xfin[k, 1].astype(F32)
        obuf[k] = total.astype(BF)
        out_copy(k).start()

    def out_copy(k):
        return pltpu.make_async_copy(obuf.at[k], out.at[pl.ds(k * PC, PC)], osem.at[k])

    def row_lse(k):
        flat = jnp.transpose(lnat[...])
        mine = jnp.zeros((2, ROWS), F32)
        for i in range(NY):
            mine = jnp.where(y == i, flat[2 * i:2 * i + 2, :], mine)
        lse_ref[...] = mine * LN2

    def run(plan):
        for f, k in plan:
            with scope(f"{f.__name__}{k}"):
                f(k)

    last_keys(0, ())
    run(((send_stats, 0),))
    last_keys(1, ((send_shares, 0),))
    run(((send_stats, 1), (join_shares, 0)))
    last_keys(2, ((send_shares, 1), (merge, 0)))
    run((
        (send_stats, 2), (join_shares, 1), (send_sums, 0), (send_shares, 2), (merge, 1),
        (join_sums, 0), (send_sums, 1), (join_shares, 2), (merge, 2), (join_sums, 1),
        (send_sums, 2), (finish, 0), (row_lse, 0), (join_sums, 2), (finish, 1), (finish, 2),
    ))
    with scope("drain"):
        for k in range(NCH):
            out_copy(k).wait()
            for copy in stat_copies(k) + scatter(k) + [mate_copy(k)] + spread(k):
                copy.wait_send()
        for copy in sent:
            copy.wait_send()


def tables():
    inverse = ROPE_BASE ** (-np.arange(HD // 2, dtype=np.float64) * 2.0 / HD)
    inverse = inverse.astype(np.float32).astype(np.float64)
    inverse = np.concatenate([inverse, inverse])
    place = np.arange(ROWS).reshape(2 * NX, NCH, PC).transpose(1, 0, 2).reshape(-1)
    local = place[:, None] * inverse[None, :]
    offset = (np.arange(NZ * NY) * ROWS)[:, None] * inverse[None, :]
    return [f(a).astype(np.float32) for a in (local, offset) for f in (np.cos, np.sin)]


DMA = pltpu.SemaphoreType.DMA


def per_device(
    tokens, norm_gain, w_query, w_key, w_value, w_outer, w_inner, w_signal,
    conv_taps, lambdas, head_gain, attend_proj, convolve_proj,
):
    rc, rs, oc, os_ = tables()
    v = pltpu.VMEM
    mixed, lse = pl.pallas_call(
        layer_kernel,
        out_shape=(
            jax.ShapeDtypeStruct((BLK, 2048), BF),
            jax.ShapeDtypeStruct((2, ROWS), F32),
        ),
        in_specs=[vmem(), pl.BlockSpec(memory_space=pltpu.SMEM)] + [vmem()] * 4 + [hbm()] * 11,
        out_specs=(hbm(), vmem()),
        scratch_shapes=[
            v((2 * NX, NCH, 2 * NX, PC, 256), BF), v((2048, HD), F32), v((ROWS, HD), F32), v((ROWS, HD), F32),
            v((6, 2048, 256), BF),
            v((256, 2048), BF), v((256, 2048), BF),
            v((ROWS + 8, 256), F32), v((ROWS, 256), F32), v((ROWS, 256), BF), v((ROWS, HD), F32),
            v((NCH, PC, 2048), BF),
            v((NY, ROWS, VD), BF), v((NZ, ROWS, 2 * VD), BF),
            v((2, NY, ROWS, HD), F32), v((2, NY, ROWS, HD), F32), v((2, NY, ROWS, VD), F32),
            v((ROWS, HD), F32), v((NY, NCH, 8, CH), F32), v((NY, ROWS, VD), BF),
            v((2, NCH * HF, VD), BF), v((2, ROWS, VD), BF),
            v((NCH, 2, NX, PC, 2048), BF), v((NCH, NX, PC, 2048), BF),
            v((NCH, 2, PC // 2, 2048), BF), v((NCH, 2, PC, 2048), BF),
            DMA((10,)), DMA((NCH,)), DMA((NCH,)), DMA((2,)), DMA((NCH, 9)), DMA((NCH, 9)),
            DMA((NCH, 6)), DMA((NCH, 6)), DMA((NCH, 6)), DMA((NCH, 6)),
            DMA((NCH, 3)), DMA((NCH, 3)), DMA((NCH, 6)), DMA((NCH, 6)),
            DMA((NCH,)), DMA((NCH,)), DMA((NCH, 6)), DMA((NCH, 6)),
        ],
        compiler_params=pltpu.CompilerParams(
            collective_id=1, has_side_effects=True, vmem_limit_bytes=62 * 2 ** 20
        ),
        name="layer",
    )(
        norm_gain.reshape(16, HD), lambdas, head_gain.reshape(1, -1), conv_taps, oc, os_,
        tokens.reshape(2 * NX, BLK, 256), rc, rs,
        w_query, w_key, w_value, w_outer, w_inner, w_signal, attend_proj, convolve_proj,
    )
    return mixed, lse.T


def solution(mesh):
    return jax.shard_map(
        per_device,
        mesh=mesh,
        in_specs=(
            P("sp", "tp"), P(), P(None, "tp"), P(None, "tp"), P(None, "tp"), P(None, "tp"),
            P(None, "tp"), P(None, "tp"), P(None, "tp"), P("tp"), P(), P("tp", None), P("tp", None),
        ),
        out_specs=(P(("sp", "tp"), None), P("sp", "tp")),
        check_vma=False,
    )
```

```python
import functools

import jax
import jax.numpy as jnp
import numpy as np
from jax import lax
from jax.experimental import pallas as pl
from jax.experimental.pallas import tpu as pltpu
from jax.sharding import PartitionSpec as P

MESH = pl.DeviceIdType.MESH
BF = jnp.bfloat16
F32 = jnp.float32
ROPE_BASE = 500000.0
NORM_EPS = 1e-05
HEAD_KEEP = 0.8
MASKED = -1e30
LOG2E = float(np.log2(np.e))
LN2 = float(np.log(2.0))
NZ, NY, NX = 4, 4, 4
ROWS = 768
HD = 128
VD = 256
CH = 256
NCH = ROWS // CH
HF = CH // 2
PC = 32
BLK = 96


def vmem():
    return pl.BlockSpec(memory_space=pltpu.VMEM)


def hbm():
    return pl.BlockSpec(memory_space=pl.ANY)


def remote(src, dst, ssem, rsem, dev):
    return pltpu.make_async_remote_copy(
        src_ref=src, dst_ref=dst, send_sem=ssem, recv_sem=rsem, device_id=dev, device_id_type=MESH
    )


def scope(name):
    return jax.named_scope(name)


def greet(devs):
    barrier = pltpu.get_barrier_semaphore()
    for dev in devs:
        pl.semaphore_signal(barrier, inc=1, device_id=dev, device_id_type=MESH)
    pl.semaphore_wait(barrier, len(devs))


def layer_kernel(
    gain, lam, hgain, taps, oc, os_, tok, rch, rsh, wq, wk, wv, wo, wi, ws, ap, cp,
    out, lse_ref,
    xbuf, gcol, rc, rs, wbuf, apb, cpb, prod, outer, conv, lnat,
    qb, kvb, m_ref, l_ref, acc, lt, stats, dbuf, relay, fin,
    part, precv, xrelay, xfin,
    wsem, tsem, bsem, send, grs, krs, qrs, trs, drs, prs, xrs,
):
    sp = lax.axis_index("sp")
    tp = lax.axis_index("tp")
    x, c = tp // 2, tp % 2
    z, y = sp // NY, sp % NY
    xr, xl, xo = lax.rem(x + 1, NX), lax.rem(x + 3, NX), lax.rem(x + 2, NX)
    yr, yl, yo = lax.rem(y + 1, NY), lax.rem(y + 3, NY), lax.rem(y + 2, NY)
    zr, zl, zo = lax.rem(z + 1, NZ), lax.rem(z + 3, NZ), lax.rem(z + 2, NZ)
    dxr, dxl, dm = (sp, xr * 2 + c), (sp, xl * 2 + c), (sp, x * 2 + (1 - c))
    dyr, dyl, dyo = (z * NY + yr, tp), (z * NY + yl, tp), (z * NY + yo, tp)
    dzr, dzl = (zr * NY + y, tp), (zl * NY + y, tp)
    dn, dp = (lax.rem(sp + 1, NZ * NY), tp), (lax.rem(sp + NZ * NY - 1, NZ * NY), tp)
    right, left, opp = xr * 2 + c, xl * 2 + c, xo * 2 + c

    tcopies = [
        pltpu.make_async_copy(tok.at[:, pl.ds(k * PC, PC), :], xbuf.at[tp, k], tsem.at[k])
        for k in range(NCH)
    ]
    for copy in tcopies:
        copy.start()
    weights = ((wk, wbuf.at[0]), (wv, wbuf.at[1]), (wq, wbuf.at[2]), (wi, wbuf.at[3]),
               (ws, wbuf.at[4]), (wo, wbuf.at[5]), (rch, rc), (rsh, rs), (ap, apb), (cp, cpb))
    wcopies = [pltpu.make_async_copy(a, b, wsem.at[i]) for i, (a, b) in enumerate(weights)]
    for copy in wcopies:
        copy.start()
    with scope("greet"):
        greet([dxr, dxl, dm, dyr, dyl, dyo, dzr, dzl, dn, dp])

    def go(copy):
        copy.start()

    def rows_of(k, h=None):
        return pl.ds(k * CH, CH) if h is None else pl.ds(k * CH + h * HF, HF)

    def pass_on(k, kind, block, h, dev):
        slot = (0, 1, 4, 2, 3, 4, 4, 4, 4)[kind]
        ref = xbuf.at[block, k] if h is None else xbuf.at[block, k, pl.ds(h * NX, NX)]
        return remote(ref, ref, send.at[0], grs.at[k, slot], dev)

    def send_own(k):
        tcopies[k].wait()
        go(pass_on(k, 0, tp, None, dxr))
        go(pass_on(k, 1, tp, None, dxl))
        go(pass_on(k, 2, tp, None, dm))

    def near(k):
        pass_on(k, 0, tp, None, dxr).wait_recv()
        go(pass_on(k, 3, left, 0, dxr))
        go(pass_on(k, 5, left, None, dm))
        pass_on(k, 1, tp, None, dxl).wait_recv()
        go(pass_on(k, 4, right, 1, dxl))
        go(pass_on(k, 6, right, None, dm))

    def far(k):
        pass_on(k, 3, left, 0, dxr).wait_recv()
        go(pass_on(k, 7, opp, 0, dm))
        pass_on(k, 4, right, 1, dxl).wait_recv()
        go(pass_on(k, 8, opp, 1, dm))

    def mates(k):
        ref = xbuf.at[pl.ds(0, NX), k]
        remote(ref, ref, send.at[0], grs.at[k, 4], dm).wait_recv()

    def ring(buf, me, lf, rt, ss, rs_, d_r, d_l):
        def one(block, k, h, kind, dev):
            ref = buf.at[block, rows_of(k, h)]
            return remote(ref, ref, ss, rs_.at[kind if kind == 6 else 2 * k + kind], dev)

        return [
            [one(me, k, None, 0, d_r), one(me, k, None, 1, d_l),
             one(lf, k, 0, 6, d_r), one(rt, k, 1, 6, d_l)]
            for k in range(NCH)
        ]

    kring = ring(kvb, z, zl, zr, send.at[1], krs, dzr, dzl)
    qring = ring(qb, y, yl, yr, send.at[2], qrs, dyr, dyl)

    def ring_send(copies):
        copies[0].start()
        copies[1].start()

    def ring_relay(copies):
        copies[0].wait_recv()
        copies[2].start()
        copies[1].wait_recv()
        copies[3].start()

    def ring_far(buf, sem, me, dev):
        remote(buf.at[me], buf.at[me], send.at[1], sem.at[6], dev).wait_recv()

    co = oc[pl.ds(sp, 1), :]
    so = os_[pl.ds(sp, 1), :]

    def compute(k):
        rows = rows_of(k)
        square = jnp.zeros((CH, HD), F32)
        blocks = [xbuf[b, k].reshape(CH, 256) for b in range(2 * NX)]
        for xb in blocks:
            xf = xb.astype(F32)
            square += xf[:, :HD] * xf[:, :HD] + xf[:, HD:] * xf[:, HD:]
        wide = jnp.concatenate(blocks, axis=1)
        total = jnp.sum(square, axis=1, keepdims=True)
        inv = lax.rsqrt(total / (2 * NX * 256) + NORM_EPS)
        c_r, s_r = rc[rows, :], rs[rows, :]
        cosine = co * c_r - so * s_r
        sine = so * c_r + co * s_r
        lane = lax.broadcasted_iota(jnp.int32, (CH, HD), 1)
        sine = jnp.where(lane < HD // 2, -sine, sine)

        def project(i):
            return inv * jnp.dot(wide, wbuf[i], preferred_element_type=F32)

        def turn(v):
            parts = []
            for j in range(2):
                t = v[:, j * HD:(j + 1) * HD]
                parts.append(t * cosine + pltpu.roll(t, HD // 2, 1) * sine)
            return jnp.concatenate(parts, axis=1)

        kvb[z, rows, 0:VD] = turn(project(0)).astype(BF)
        kvb[z, rows, VD:2 * VD] = project(1).astype(BF)
        qb[y, rows, :] = (turn(project(2)) * (LOG2E * HD ** -0.5)).astype(BF)
        pr = project(3) * project(4)
        og = project(5)
        for t in range(2 * NX):
            at = t * BLK + k * PC
            prod[8 + at:8 + at + PC, :] = pr[t * PC:(t + 1) * PC]
            outer[at:at + PC, :] = og[t * PC:(t + 1) * PC]
        ring_send(kring[k])
        ring_send(qring[k])

    def scores(qi, kj, rows, j):
        q = qb[qi, rows, j * HD:(j + 1) * HD]
        k = kvb[kj, :, j * HD:(j + 1) * HD]
        return lax.dot_general(q, k, (((1,), (1,)), ((), ())), preferred_element_type=F32)

    def absorb(qi, kj, rows, j, s):
        before = m_ref[j, qi, rows, :]
        now = jnp.maximum(before, jnp.max(s, axis=1, keepdims=True))
        fade = jnp.exp2(before - now)
        p = jnp.exp2(s - jnp.concatenate([now] * (ROWS // HD), axis=1))
        total = l_ref[j, qi, rows, :] * fade
        for i in range(ROWS // HD):
            total = total + p[:, i * HD:(i + 1) * HD]
        l_ref[j, qi, rows, :] = total
        m_ref[j, qi, rows, :] = now
        acc[j, qi, rows, :] = acc[j, qi, rows, :] * jnp.concatenate([fade] * 2, axis=1) + jnp.dot(
            p.astype(BF), kvb[kj, :, VD:2 * VD], preferred_element_type=F32
        )

    def attend(qi, kj, rows, mask=None):
        ss = [scores(qi, kj, rows, j) for j in range(2)]
        for j in range(2):
            s = ss[j] if mask is None else jnp.where(mask, ss[j], MASKED)
            absorb(qi, kj, rows, j, s)

    def place(p):
        return ((p >> 5) & 7) * BLK + (p >> 8) * PC + (p & 31)

    def own_pair():
        row = place(lax.broadcasted_iota(jnp.int32, (ROWS, HD), 0))
        row = jnp.concatenate([row] * (ROWS // HD), axis=1)
        col = place(lax.broadcasted_iota(jnp.int32, (1, ROWS), 1))
        attend(y, z, pl.ds(0, ROWS), col <= row)

    def scale_weights():
        g = jnp.concatenate([gain[...], jnp.zeros((HD - 16, HD), F32)], axis=0)
        g = jnp.transpose(g)
        for b in range(16):
            gcol[b * HD:(b + 1) * HD, :] = jnp.broadcast_to(g[:, b:b + 1], (HD, HD))

        def one(i, _):
            for b in range(8):
                rows = slice(b * 256, (b + 1) * 256)
                col = gcol[rows, :]
                w = wbuf[i, rows, :].astype(F32)
                wbuf[i, rows, :] = (w * jnp.concatenate([col, col], axis=1)).astype(BF)
            return 0

        lax.fori_loop(0, 6, one, 0)

    def start():
        m_ref[...] = jnp.full(m_ref.shape, MASKED, F32)
        l_ref[...] = jnp.zeros(l_ref.shape, F32)
        acc[...] = jnp.zeros(acc.shape, F32)

    send_own(0)
    send_own(1)
    with scope("init"):
        start()
        for copy in wcopies:
            copy.wait()
    with scope("scale"):
        scale_weights()
    with scope("near0"):
        near(0)
    with scope("near1"):
        near(1)
    send_own(2)
    with scope("far0"):
        far(0)
    with scope("near2"):
        near(2)
    with scope("mates0"):
        mates(0)
    with scope("comp0"):
        compute(0)
    with scope("far1"):
        far(1)
    with scope("far2"):
        far(2)
    with scope("mates1"):
        mates(1)
    with scope("comp1"):
        compute(1)
    with scope("mates2"):
        mates(2)
    with scope("qrel0"):
        ring_relay(qring[0])
    with scope("comp2"):
        compute(2)
    border = remote(prod.at[pl.ds(ROWS, 8)], prod.at[pl.ds(0, 8)], bsem.at[0], bsem.at[1], dn)
    border.start()
    with scope("own"):
        own_pair()
    with scope("rel0"):
        ring_relay(kring[0])
        ring_relay(qring[1])
    with scope("conv"):
        border.wait_recv()

        @pl.when(sp == 0)
        def _():
            prod[0:8, :] = jnp.zeros((8, 256), F32)

        tv = taps[...].astype(F32)
        smoothed = (
            tv[0:1] * prod[6:6 + ROWS, :] + tv[1:2] * prod[7:7 + ROWS, :] + tv[2:3] * prod[8:8 + ROWS, :]
        )
        conv[...] = (outer[...] * smoothed).astype(BF)
    with scope("qrel2"):
        ring_relay(qring[2])
    with scope("rel1"):
        ring_relay(kring[1])

    def step(i, _):
        @pl.when(i == 2)
        def _():
            with scope("qfar"):
                ring_far(qb, qrs, y, dyr)

        @pl.when(i == 3)
        def _():
            with scope("rel2"):
                ring_relay(kring[2])

        mine = i < 3
        turn_ = jnp.where(i == 0, 1, jnp.where(i == 1, 3, 2))
        qi = jnp.where(mine, lax.rem(y + turn_, NY), lax.rem(i + 1, NY))
        kj = jnp.where(mine, z, zl)
        need = (mine & (qi > y)) | (~mine & (z >= 1))

        @pl.when(need)
        def _():
            with scope("item"):
                attend(qi, kj, pl.ds(0, ROWS))

        return 0

    lax.fori_loop(0, 7, step, 0)
    lam_v = lam[0]

    def last_keys(k, between):
        def body(i, _):
            right_turn = i == 0
            if k == 0:
                @pl.when(i == 1)
                def _():
                    with scope("kfar"):
                        ring_far(kvb, krs, z, dzr)

            kj = jnp.where(right_turn, zr, zo)

            @pl.when((z == 3) | ((i == 1) & (z == 2)))
            def _():
                with scope("tiles"):
                    ss = [[scores(qi, kj, rows_of(k), j) for qi in range(NY)] for j in range(2)]
                    for j in range(2):
                        for qi in range(NY):
                            absorb(qi, kj, rows_of(k), j, ss[j][qi])

            if between:
                @pl.when(right_turn)
                def _():
                    for f, kk in between:
                        with scope(f"{f.__name__}{kk}"):
                            f(kk)

            return 0

        lax.fori_loop(0, 2, body, 0)

    def stat_copies(k):
        ref = stats.at[y, k]
        return [
            remote(ref, ref, send.at[3], trs.at[k], dev) for dev in (dyr, dyl, dyo)
        ]

    def send_stats(k):
        rows = rows_of(k)
        lane = lax.broadcasted_iota(jnp.int32, (CH, HD), 1)
        table = jnp.full((CH, HD), MASKED, F32)
        for qi in range(NY):
            for j in range(2):
                total = jnp.sum(l_ref[j, qi, rows, :], axis=1, keepdims=True)
                lse = m_ref[j, qi, rows, :] + jnp.log2(jnp.maximum(total, 1e-37))
                table = jnp.where(lane == 2 * qi + j, lse, table)
        stats[y, k] = jnp.transpose(table)[0:8, :]
        for copy in stat_copies(k):
            copy.start()

    def pick(rows, qi, j):
        lanes = lax.broadcasted_iota(jnp.int32, (CH, HD), 1)
        return jnp.sum(jnp.where(lanes == 2 * qi + j, lt[rows, :], 0.0), axis=1, keepdims=True)

    def share(rows, qi):
        outs = []
        for j in range(2):
            f = jnp.exp2(m_ref[j, qi, rows, :] - pick(rows, qi, j))
            outs.append(acc[j, qi, rows, :] * jnp.concatenate([f] * 2, axis=1))
        return outs[0] - lam_v * outs[1]

    def scatter(k):
        h0, h1 = rows_of(k, 0), rows_of(k, 1)
        at = pl.ds(k * HF, HF)
        pairs = [
            (dbuf.at[yo, h0], relay.at[0, at], dyr),
            (dbuf.at[yo, h1], relay.at[1, at], dyl),
            (dbuf.at[yr, h1], fin.at[0, h1], dyr),
            (dbuf.at[yl, h0], fin.at[1, h0], dyl),
            (dbuf.at[yr, h0], fin.at[0, h0], dyr),
            (dbuf.at[yl, h1], fin.at[1, h1], dyl),
        ]
        return [
            remote(a, b, send.at[4], drs.at[k, min(i, 2)], d) for i, (a, b, d) in enumerate(pairs)
        ]

    def send_shares(k):
        rows = rows_of(k)
        ref = stats.at[pl.ds(0, NY - 1), k]
        remote(ref, ref, send.at[3], trs.at[k], dyr).wait_recv()
        parts = [stats[i, k] for i in range(NY)]
        peak = jnp.maximum(jnp.maximum(parts[0], parts[1]), jnp.maximum(parts[2], parts[3]))
        whole = peak + jnp.log2(sum(jnp.exp2(p - peak) for p in parts))
        lt[rows, :] = jnp.transpose(jnp.concatenate([whole, jnp.zeros((HD - 8, CH), F32)], axis=0))

        def one(i, _):
            qi = lax.rem(y + jnp.where(i == 0, 2, jnp.where(i == 1, 1, 3)), NY)
            dbuf[qi, rows, :] = share(rows, qi).astype(BF)
            return 0

        lax.fori_loop(0, NY - 1, one, 0)
        for copy in scatter(k)[:4]:
            copy.start()

    def join_shares(k):
        copies = scatter(k)
        h0, h1 = rows_of(k, 0), rows_of(k, 1)
        at = pl.ds(k * HF, HF)
        copies[0].wait_recv()
        dbuf[yr, h0, :] = (dbuf[yr, h0, :].astype(F32) + relay[0, at, :].astype(F32)).astype(BF)
        copies[4].start()
        copies[1].wait_recv()
        dbuf[yl, h1, :] = (dbuf[yl, h1, :].astype(F32) + relay[1, at, :].astype(F32)).astype(BF)
        copies[5].start()

    def mate_copy(k):
        return remote(part.at[k, 1 - c], precv.at[k], send.at[5], prs.at[k], dm)

    def merge(k):
        rows = rows_of(k)
        ref = fin.at[:, rows]
        remote(ref, ref, send.at[4], drs.at[k, 2], dyr).wait_recv()
        d = share(rows, y) + fin[0, rows, :].astype(F32) + fin[1, rows, :].astype(F32)
        back = lax.rsqrt(jnp.mean(d * d, axis=1, keepdims=True) + NORM_EPS)
        att = (d * back * hgain[...] * HEAD_KEEP).astype(BF)
        pieces = [slice(t * BLK + k * PC, t * BLK + (k + 1) * PC) for t in range(2 * NX)]
        for t in range(2 * NX):
            lnat[pieces[t], :] = lt[k * CH + t * PC:k * CH + (t + 1) * PC, :]
        con = jnp.concatenate([conv[pieces[t], :] for t in range(2 * NX)], axis=0)
        cols = 512
        for n in range(2048 // cols):
            cs = slice(n * cols, (n + 1) * cols)
            p = jnp.dot(att, apb[:, cs], preferred_element_type=F32) + jnp.dot(
                con, cpb[:, cs], preferred_element_type=F32
            )
            p = p.astype(BF)
            for t in range(2 * NX):
                part[k, t % 2, t // 2, :, cs] = p[t * PC:(t + 1) * PC]
        mate_copy(k).start()

    g0, g1 = pl.ds(0, PC // 2), pl.ds(PC // 2, PC // 2)

    def spread(k):
        pairs = [
            (part.at[k, c, xo, g0], xrelay.at[k, 0], dxr),
            (part.at[k, c, xo, g1], xrelay.at[k, 1], dxl),
            (part.at[k, c, xr, g1], xfin.at[k, 0, g1], dxr),
            (part.at[k, c, xl, g0], xfin.at[k, 1, g0], dxl),
            (part.at[k, c, xr, g0], xfin.at[k, 0, g0], dxr),
            (part.at[k, c, xl, g1], xfin.at[k, 1, g1], dxl),
        ]
        return [
            remote(a, b, send.at[6], xrs.at[k, min(i, 2)], d) for i, (a, b, d) in enumerate(pairs)
        ]

    def add_mate(k, xx, g, extra=None):
        t = part[k, c, xx, g, :].astype(F32) + precv[k, xx, g, :].astype(F32)
        if extra is not None:
            t = t + extra.astype(F32)
        part[k, c, xx, g, :] = t.astype(BF)

    def send_sums(k):
        copies = spread(k)
        mate_copy(k).wait_recv()
        add_mate(k, xo, pl.ds(0, PC))
        add_mate(k, xr, g1)
        add_mate(k, xl, g0)
        for copy in copies[:4]:
            copy.start()

    def join_sums(k):
        copies = spread(k)
        copies[0].wait_recv()
        add_mate(k, xr, g0, xrelay[k, 0])
        copies[4].start()
        copies[1].wait_recv()
        add_mate(k, xl, g1, xrelay[k, 1])
        copies[5].start()

    def finish(k):
        remote(xfin.at[k], xfin.at[k], send.at[6], xrs.at[k, 2], dxr).wait_recv()
        total = part[k, c, x].astype(F32) + precv[k, x].astype(F32)
        total = total + xfin[k, 0].astype(F32) + xfin[k, 1].astype(F32)
        out[k * PC:(k + 1) * PC, :] = total.astype(BF)

    def row_lse(k):
        flat = jnp.transpose(lnat[...])
        mine = jnp.zeros((2, ROWS), F32)
        for i in range(NY):
            mine = jnp.where(y == i, flat[2 * i:2 * i + 2, :], mine)
        lse_ref[...] = mine * LN2

    def run(plan):
        for f, k in plan:
            with scope(f"{f.__name__}{k}"):
                f(k)

    last_keys(0, ())
    run(((send_stats, 0),))
    last_keys(1, ((send_shares, 0),))
    run(((send_stats, 1), (join_shares, 0)))
    last_keys(2, ((send_shares, 1), (merge, 0)))
    run((
        (send_stats, 2), (join_shares, 1), (send_sums, 0), (send_shares, 2), (merge, 1),
        (join_sums, 0), (send_sums, 1), (join_shares, 2), (merge, 2), (join_sums, 1),
        (send_sums, 2), (finish, 0), (row_lse, 0), (join_sums, 2), (finish, 1), (finish, 2),
    ))
    with scope("drain"):
        groups = (xbuf.at[pl.ds(0, 7)], kvb.at[pl.ds(0, 3)], qb.at[pl.ds(0, 3)],
                  stats.at[pl.ds(0, 3)], dbuf.at[pl.ds(0, 3)], precv, part.at[:, 0, pl.ds(0, 3)])
        for i, ref in enumerate(groups):
            remote(ref, ref, send.at[i], grs.at[0, 0], dm).wait_send()
        border.wait_send()


def tables():
    inverse = ROPE_BASE ** (-np.arange(HD // 2, dtype=np.float64) * 2.0 / HD)
    inverse = inverse.astype(np.float32).astype(np.float64)
    inverse = np.concatenate([inverse, inverse])
    place = np.arange(ROWS).reshape(2 * NX, NCH, PC).transpose(1, 0, 2).reshape(-1)
    local = place[:, None] * inverse[None, :]
    offset = (np.arange(NZ * NY) * ROWS)[:, None] * inverse[None, :]
    return [f(a).astype(np.float32) for a in (local, offset) for f in (np.cos, np.sin)]


DMA = pltpu.SemaphoreType.DMA


def per_device(
    tokens, norm_gain, w_query, w_key, w_value, w_outer, w_inner, w_signal,
    conv_taps, lambdas, head_gain, attend_proj, convolve_proj,
):
    rc, rs, oc, os_ = tables()
    v = pltpu.VMEM
    mixed, lse = pl.pallas_call(
        layer_kernel,
        out_shape=(
            jax.ShapeDtypeStruct((BLK, 2048), BF),
            jax.ShapeDtypeStruct((2, ROWS), F32),
        ),
        in_specs=[vmem(), pl.BlockSpec(memory_space=pltpu.SMEM)] + [vmem()] * 4 + [hbm()] * 11,
        out_specs=(vmem(), vmem()),
        scratch_shapes=[
            v((2 * NX, NCH, 2 * NX, PC, 256), BF), v((2048, HD), F32), v((ROWS, HD), F32), v((ROWS, HD), F32),
            v((6, 2048, 256), BF),
            v((256, 2048), BF), v((256, 2048), BF),
            v((ROWS + 8, 256), F32), v((ROWS, 256), F32), v((ROWS, 256), BF), v((ROWS, HD), F32),
            v((NY, ROWS, VD), BF), v((NZ, ROWS, 2 * VD), BF),
            v((2, NY, ROWS, HD), F32), v((2, NY, ROWS, HD), F32), v((2, NY, ROWS, VD), F32),
            v((ROWS, HD), F32), v((NY, NCH, 8, CH), F32), v((NY, ROWS, VD), BF),
            v((2, NCH * HF, VD), BF), v((2, ROWS, VD), BF),
            v((NCH, 2, NX, PC, 2048), BF), v((NCH, NX, PC, 2048), BF),
            v((NCH, 2, PC // 2, 2048), BF), v((NCH, 2, PC, 2048), BF),
            DMA((10,)), DMA((NCH,)), DMA((2,)), DMA((7,)), DMA((NCH, 5)), DMA((7,)), DMA((7,)),
            DMA((NCH,)), DMA((NCH, 3)), DMA((NCH,)), DMA((NCH, 3)),
        ],
        compiler_params=pltpu.CompilerParams(
            collective_id=1, has_side_effects=True, vmem_limit_bytes=62 * 2 ** 20
        ),
        name="layer",
    )(
        norm_gain.reshape(16, HD), lambdas, head_gain.reshape(1, -1), conv_taps, oc, os_,
        tokens.reshape(2 * NX, BLK, 256), rc, rs,
        w_query, w_key, w_value, w_outer, w_inner, w_signal, attend_proj, convolve_proj,
    )
    return mixed, lse.T


def solution(mesh):
    return jax.shard_map(
        per_device,
        mesh=mesh,
        in_specs=(
            P("sp", "tp"), P(), P(None, "tp"), P(None, "tp"), P(None, "tp"), P(None, "tp"),
            P(None, "tp"), P(None, "tp"), P(None, "tp"), P("tp"), P(), P("tp", None), P("tp", None),
        ),
        out_specs=(P(("sp", "tp"), None), P("sp", "tp")),
        check_vma=False,
    )
```

```python
import functools

import jax
import jax.numpy as jnp
import numpy as np
from jax import lax
from jax.experimental import pallas as pl
from jax.experimental.pallas import tpu as pltpu
from jax.sharding import PartitionSpec as P

MESH = pl.DeviceIdType.MESH
BF = jnp.bfloat16
F32 = jnp.float32
ROPE_BASE = 500000.0
NORM_EPS = 1e-05
HEAD_KEEP = 0.8
MASKED = -1e30
LOG2E = float(np.log2(np.e))
LN2 = float(np.log(2.0))
NZ, NY, NX = 4, 4, 4
ROWS = 768
HD = 128
VD = 256
CH = 256
NCH = ROWS // CH
HF = CH // 2
PC = 32
BLK = 96


def vmem():
    return pl.BlockSpec(memory_space=pltpu.VMEM)


def hbm():
    return pl.BlockSpec(memory_space=pl.ANY)


def remote(src, dst, ssem, rsem, dev):
    return pltpu.make_async_remote_copy(
        src_ref=src, dst_ref=dst, send_sem=ssem, recv_sem=rsem, device_id=dev, device_id_type=MESH
    )


def scope(name):
    return jax.named_scope(name)


def greet(devs):
    barrier = pltpu.get_barrier_semaphore()
    for dev in devs:
        pl.semaphore_signal(barrier, inc=1, device_id=dev, device_id_type=MESH)
    pl.semaphore_wait(barrier, len(devs))


def layer_kernel(
    gain, lam, hgain, taps, oc, os_, tok, rch, rsh, wq, wk, wv, wo, wi, ws, ap, cp,
    out, lse_ref,
    xbuf, gcol, rc, rs, wbuf, apb, cpb, prod, outer, conv, lnat,
    qb, kvb, m_ref, l_ref, acc, lt, stats, dbuf, relay, fin,
    part, precv, xrelay, xfin,
    wsem, tsem, bsem, send, grs, krs, qrs, trs, drs, prs, xrs,
):
    sp = lax.axis_index("sp")
    tp = lax.axis_index("tp")
    x, c = tp // 2, tp % 2
    z, y = sp // NY, sp % NY
    xr, xl, xo = lax.rem(x + 1, NX), lax.rem(x + 3, NX), lax.rem(x + 2, NX)
    yr, yl, yo = lax.rem(y + 1, NY), lax.rem(y + 3, NY), lax.rem(y + 2, NY)
    zr, zl, zo = lax.rem(z + 1, NZ), lax.rem(z + 3, NZ), lax.rem(z + 2, NZ)
    dxr, dxl, dm = (sp, xr * 2 + c), (sp, xl * 2 + c), (sp, x * 2 + (1 - c))
    dyr, dyl, dyo = (z * NY + yr, tp), (z * NY + yl, tp), (z * NY + yo, tp)
    dzr, dzl = (zr * NY + y, tp), (zl * NY + y, tp)
    dn, dp = (lax.rem(sp + 1, NZ * NY), tp), (lax.rem(sp + NZ * NY - 1, NZ * NY), tp)
    right, left, opp = xr * 2 + c, xl * 2 + c, xo * 2 + c

    tcopies = [
        pltpu.make_async_copy(tok.at[:, pl.ds(k * PC, PC), :], xbuf.at[tp, k], tsem.at[k])
        for k in range(NCH)
    ]
    for copy in tcopies:
        copy.start()
    weights = ((wk, wbuf.at[0]), (wv, wbuf.at[1]), (wq, wbuf.at[2]), (wi, wbuf.at[3]),
               (ws, wbuf.at[4]), (wo, wbuf.at[5]), (rch, rc), (rsh, rs), (ap, apb), (cp, cpb))
    wcopies = [pltpu.make_async_copy(a, b, wsem.at[i]) for i, (a, b) in enumerate(weights)]
    for copy in wcopies:
        copy.start()
    with scope("greet"):
        greet([dxr, dxl, dm, dyr, dyl, dyo, dzr, dzl, dn, dp])

    def go(copy):
        copy.start()

    def rows_of(k, h=None):
        return pl.ds(k * CH, CH) if h is None else pl.ds(k * CH + h * HF, HF)

    def pass_on(k, kind, block, h, dev):
        slot = (0, 1, 4, 2, 3, 4, 4, 4, 4)[kind]
        ref = xbuf.at[block, k] if h is None else xbuf.at[block, k, pl.ds(h * NX, NX)]
        return remote(ref, ref, send.at[0], grs.at[k, slot], dev)

    def send_own(k):
        tcopies[k].wait()
        go(pass_on(k, 0, tp, None, dxr))
        go(pass_on(k, 1, tp, None, dxl))
        go(pass_on(k, 2, tp, None, dm))

    def near(k):
        pass_on(k, 0, tp, None, dxr).wait_recv()
        go(pass_on(k, 3, left, 0, dxr))
        go(pass_on(k, 5, left, None, dm))
        pass_on(k, 1, tp, None, dxl).wait_recv()
        go(pass_on(k, 4, right, 1, dxl))
        go(pass_on(k, 6, right, None, dm))

    def far(k):
        pass_on(k, 3, left, 0, dxr).wait_recv()
        go(pass_on(k, 7, opp, 0, dm))
        pass_on(k, 4, right, 1, dxl).wait_recv()
        go(pass_on(k, 8, opp, 1, dm))

    def mates(k):
        ref = xbuf.at[pl.ds(0, NX), k]
        remote(ref, ref, send.at[0], grs.at[k, 4], dm).wait_recv()

    def ring(buf, me, lf, rt, ss, rs_, d_r, d_l):
        def one(block, k, h, kind, dev):
            ref = buf.at[block, rows_of(k, h)]
            return remote(ref, ref, ss, rs_.at[kind if kind == 6 else 2 * k + kind], dev)

        return [
            [one(me, k, None, 0, d_r), one(me, k, None, 1, d_l),
             one(lf, k, 0, 6, d_r), one(rt, k, 1, 6, d_l)]
            for k in range(NCH)
        ]

    kring = ring(kvb, z, zl, zr, send.at[1], krs, dzr, dzl)
    qring = ring(qb, y, yl, yr, send.at[2], qrs, dyr, dyl)

    def ring_send(copies):
        copies[0].start()
        copies[1].start()

    def ring_relay(copies):
        copies[0].wait_recv()
        copies[2].start()
        copies[1].wait_recv()
        copies[3].start()

    def ring_far(buf, sem, me, dev):
        remote(buf.at[me], buf.at[me], send.at[1], sem.at[6], dev).wait_recv()

    border = remote(prod.at[pl.ds(ROWS, 8)], prod.at[pl.ds(0, 8)], bsem.at[0], bsem.at[1], dn)
    co = oc[pl.ds(sp, 1), :]
    so = os_[pl.ds(sp, 1), :]

    def compute(k):
        rows = rows_of(k)
        square = jnp.zeros((CH, HD), F32)
        blocks = [xbuf[b, k].reshape(CH, 256) for b in range(2 * NX)]
        for xb in blocks:
            xf = xb.astype(F32)
            square += xf[:, :HD] * xf[:, :HD] + xf[:, HD:] * xf[:, HD:]
        wide = jnp.concatenate(blocks, axis=1)
        total = jnp.sum(square, axis=1, keepdims=True)
        inv = lax.rsqrt(total / (2 * NX * 256) + NORM_EPS)
        c_r, s_r = rc[rows, :], rs[rows, :]
        cosine = co * c_r - so * s_r
        sine = so * c_r + co * s_r
        lane = lax.broadcasted_iota(jnp.int32, (CH, HD), 1)
        sine = jnp.where(lane < HD // 2, -sine, sine)

        def project(i):
            return inv * jnp.dot(wide, wbuf[i], preferred_element_type=F32)

        def turn(v):
            parts = []
            for j in range(2):
                t = v[:, j * HD:(j + 1) * HD]
                parts.append(t * cosine + pltpu.roll(t, HD // 2, 1) * sine)
            return jnp.concatenate(parts, axis=1)

        kvb[z, rows, 0:VD] = turn(project(0)).astype(BF)
        kvb[z, rows, VD:2 * VD] = project(1).astype(BF)
        qb[y, rows, :] = (turn(project(2)) * (LOG2E * HD ** -0.5)).astype(BF)
        pr = project(3) * project(4)
        og = project(5)
        for t in range(2 * NX):
            at = t * BLK + k * PC
            prod[8 + at:8 + at + PC, :] = pr[t * PC:(t + 1) * PC]
            outer[at:at + PC, :] = og[t * PC:(t + 1) * PC]
        if k == NCH - 1:
            border.start()
        ring_send(kring[k])
        ring_send(qring[k])

    def scores(qi, kj, rows, j):
        q = qb[qi, rows, j * HD:(j + 1) * HD]
        k = kvb[kj, :, j * HD:(j + 1) * HD]
        return lax.dot_general(q, k, (((1,), (1,)), ((), ())), preferred_element_type=F32)

    def absorb(qi, kj, rows, j, s):
        before = m_ref[j, qi, rows, :]
        now = jnp.maximum(before, jnp.max(s, axis=1, keepdims=True))
        fade = jnp.exp2(before - now)
        p = jnp.exp2(s - jnp.concatenate([now] * (ROWS // HD), axis=1))
        total = l_ref[j, qi, rows, :] * fade
        for i in range(ROWS // HD):
            total = total + p[:, i * HD:(i + 1) * HD]
        l_ref[j, qi, rows, :] = total
        m_ref[j, qi, rows, :] = now
        acc[j, qi, rows, :] = acc[j, qi, rows, :] * jnp.concatenate([fade] * 2, axis=1) + jnp.dot(
            p.astype(BF), kvb[kj, :, VD:2 * VD], preferred_element_type=F32
        )

    def attend(qi, kj, rows, mask=None):
        ss = [scores(qi, kj, rows, j) for j in range(2)]
        for j in range(2):
            s = ss[j] if mask is None else jnp.where(mask, ss[j], MASKED)
            absorb(qi, kj, rows, j, s)

    def place(p):
        return ((p >> 5) & 7) * BLK + (p >> 8) * PC + (p & 31)

    def own_pair():
        row = place(lax.broadcasted_iota(jnp.int32, (ROWS, HD), 0))
        row = jnp.concatenate([row] * (ROWS // HD), axis=1)
        col = place(lax.broadcasted_iota(jnp.int32, (1, ROWS), 1))
        attend(y, z, pl.ds(0, ROWS), col <= row)

    def scale_weights():
        g = jnp.concatenate([gain[...], jnp.zeros((HD - 16, HD), F32)], axis=0)
        g = jnp.transpose(g)
        for b in range(16):
            gcol[b * HD:(b + 1) * HD, :] = jnp.broadcast_to(g[:, b:b + 1], (HD, HD))

        def one(i, _):
            for b in range(8):
                rows = slice(b * 256, (b + 1) * 256)
                col = gcol[rows, :]
                w = wbuf[i, rows, :].astype(F32)
                wbuf[i, rows, :] = (w * jnp.concatenate([col, col], axis=1)).astype(BF)
            return 0

        lax.fori_loop(0, 6, one, 0)

    def start():
        m_ref[...] = jnp.full(m_ref.shape, MASKED, F32)
        l_ref[...] = jnp.zeros(l_ref.shape, F32)
        acc[...] = jnp.zeros(acc.shape, F32)

    send_own(0)
    send_own(1)
    with scope("init"):
        start()
        for copy in wcopies:
            copy.wait()
    with scope("scale"):
        scale_weights()
    with scope("near0"):
        near(0)
    with scope("near1"):
        near(1)
    send_own(2)
    with scope("far0"):
        far(0)
    with scope("mates0"):
        mates(0)
    with scope("comp0"):
        compute(0)
    with scope("near2"):
        near(2)
    with scope("far1"):
        far(1)
    with scope("mates1"):
        mates(1)
    with scope("comp1"):
        compute(1)
    with scope("far2"):
        far(2)
    with scope("mates2"):
        mates(2)
    with scope("qrel0"):
        ring_relay(qring[0])
    with scope("comp2"):
        compute(2)
    with scope("own"):
        own_pair()
    with scope("conv"):
        border.wait_recv()

        @pl.when(sp == 0)
        def _():
            prod[0:8, :] = jnp.zeros((8, 256), F32)

        tv = taps[...].astype(F32)
        smoothed = (
            tv[0:1] * prod[6:6 + ROWS, :] + tv[1:2] * prod[7:7 + ROWS, :] + tv[2:3] * prod[8:8 + ROWS, :]
        )
        conv[...] = (outer[...] * smoothed).astype(BF)
    with scope("qrel1"):
        ring_relay(qring[1])
    with scope("rel0"):
        ring_relay(kring[0])
    with scope("qrel2"):
        ring_relay(qring[2])
    with scope("rel1"):
        ring_relay(kring[1])

    def step(i, _):
        @pl.when(i == 2)
        def _():
            with scope("qfar"):
                ring_far(qb, qrs, y, dyr)

        @pl.when(i == 3)
        def _():
            with scope("rel2"):
                ring_relay(kring[2])

        mine = i < 3
        turn_ = jnp.where(i == 0, 1, jnp.where(i == 1, 3, 2))
        qi = jnp.where(mine, lax.rem(y + turn_, NY), lax.rem(i + 1, NY))
        kj = jnp.where(mine, z, zl)
        need = (mine & (qi > y)) | (~mine & (z >= 1))

        @pl.when(need)
        def _():
            with scope("item"):
                attend(qi, kj, pl.ds(0, ROWS))

        return 0

    lax.fori_loop(0, 7, step, 0)
    lam_v = lam[0]

    def last_keys(k, between):
        def body(i, _):
            right_turn = i == 0
            if k == 0:
                @pl.when(i == 1)
                def _():
                    with scope("kfar"):
                        ring_far(kvb, krs, z, dzr)

            kj = jnp.where(right_turn, zr, zo)

            @pl.when((z == 3) | ((i == 1) & (z == 2)))
            def _():
                with scope("tiles"):
                    ss = [[scores(qi, kj, rows_of(k), j) for qi in range(NY)] for j in range(2)]
                    for j in range(2):
                        for qi in range(NY):
                            absorb(qi, kj, rows_of(k), j, ss[j][qi])

            if between:
                @pl.when(right_turn)
                def _():
                    for f, kk in between:
                        with scope(f"{f.__name__}{kk}"):
                            f(kk)

            return 0

        lax.fori_loop(0, 2, body, 0)

    def stat_copies(k):
        ref = stats.at[y, k]
        return [
            remote(ref, ref, send.at[3], trs.at[k], dev) for dev in (dyr, dyl, dyo)
        ]

    def send_stats(k):
        rows = rows_of(k)
        lane = lax.broadcasted_iota(jnp.int32, (CH, HD), 1)
        table = jnp.full((CH, HD), MASKED, F32)
        for qi in range(NY):
            for j in range(2):
                total = jnp.sum(l_ref[j, qi, rows, :], axis=1, keepdims=True)
                lse = m_ref[j, qi, rows, :] + jnp.log2(jnp.maximum(total, 1e-37))
                table = jnp.where(lane == 2 * qi + j, lse, table)
        stats[y, k] = jnp.transpose(table)[0:8, :]
        for copy in stat_copies(k):
            copy.start()

    def pick(rows, qi, j):
        lanes = lax.broadcasted_iota(jnp.int32, (CH, HD), 1)
        return jnp.sum(jnp.where(lanes == 2 * qi + j, lt[rows, :], 0.0), axis=1, keepdims=True)

    def share(rows, qi):
        outs = []
        for j in range(2):
            f = jnp.exp2(m_ref[j, qi, rows, :] - pick(rows, qi, j))
            outs.append(acc[j, qi, rows, :] * jnp.concatenate([f] * 2, axis=1))
        return outs[0] - lam_v * outs[1]

    def scatter(k):
        h0, h1 = rows_of(k, 0), rows_of(k, 1)
        at = pl.ds(k * HF, HF)
        pairs = [
            (dbuf.at[yo, h0], relay.at[0, at], dyr),
            (dbuf.at[yo, h1], relay.at[1, at], dyl),
            (dbuf.at[yr, h1], fin.at[0, h1], dyr),
            (dbuf.at[yl, h0], fin.at[1, h0], dyl),
            (dbuf.at[yr, h0], fin.at[0, h0], dyr),
            (dbuf.at[yl, h1], fin.at[1, h1], dyl),
        ]
        return [
            remote(a, b, send.at[4], drs.at[k, min(i, 2)], d) for i, (a, b, d) in enumerate(pairs)
        ]

    def send_shares(k):
        rows = rows_of(k)
        ref = stats.at[pl.ds(0, NY - 1), k]
        remote(ref, ref, send.at[3], trs.at[k], dyr).wait_recv()
        parts = [stats[i, k] for i in range(NY)]
        peak = jnp.maximum(jnp.maximum(parts[0], parts[1]), jnp.maximum(parts[2], parts[3]))
        whole = peak + jnp.log2(sum(jnp.exp2(p - peak) for p in parts))
        lt[rows, :] = jnp.transpose(jnp.concatenate([whole, jnp.zeros((HD - 8, CH), F32)], axis=0))

        def one(i, _):
            qi = lax.rem(y + jnp.where(i == 0, 2, jnp.where(i == 1, 1, 3)), NY)
            dbuf[qi, rows, :] = share(rows, qi).astype(BF)
            return 0

        lax.fori_loop(0, NY - 1, one, 0)
        for copy in scatter(k)[:4]:
            copy.start()

    def join_shares(k):
        copies = scatter(k)
        h0, h1 = rows_of(k, 0), rows_of(k, 1)
        at = pl.ds(k * HF, HF)
        copies[0].wait_recv()
        dbuf[yr, h0, :] = (dbuf[yr, h0, :].astype(F32) + relay[0, at, :].astype(F32)).astype(BF)
        copies[4].start()
        copies[1].wait_recv()
        dbuf[yl, h1, :] = (dbuf[yl, h1, :].astype(F32) + relay[1, at, :].astype(F32)).astype(BF)
        copies[5].start()

    def mate_copy(k):
        return remote(part.at[k, 1 - c], precv.at[k], send.at[5], prs.at[k], dm)

    def merge(k):
        rows = rows_of(k)
        ref = fin.at[:, rows]
        remote(ref, ref, send.at[4], drs.at[k, 2], dyr).wait_recv()
        d = share(rows, y) + fin[0, rows, :].astype(F32) + fin[1, rows, :].astype(F32)
        back = lax.rsqrt(jnp.mean(d * d, axis=1, keepdims=True) + NORM_EPS)
        att = (d * back * hgain[...] * HEAD_KEEP).astype(BF)
        pieces = [slice(t * BLK + k * PC, t * BLK + (k + 1) * PC) for t in range(2 * NX)]
        for t in range(2 * NX):
            lnat[pieces[t], :] = lt[k * CH + t * PC:k * CH + (t + 1) * PC, :]
        con = jnp.concatenate([conv[pieces[t], :] for t in range(2 * NX)], axis=0)
        cols = 512
        for n in range(2048 // cols):
            cs = slice(n * cols, (n + 1) * cols)
            p = jnp.dot(att, apb[:, cs], preferred_element_type=F32) + jnp.dot(
                con, cpb[:, cs], preferred_element_type=F32
            )
            p = p.astype(BF)
            for t in range(2 * NX):
                part[k, t % 2, t // 2, :, cs] = p[t * PC:(t + 1) * PC]
        mate_copy(k).start()

    g0, g1 = pl.ds(0, PC // 2), pl.ds(PC // 2, PC // 2)

    def spread(k):
        pairs = [
            (part.at[k, c, xo, g0], xrelay.at[k, 0], dxr),
            (part.at[k, c, xo, g1], xrelay.at[k, 1], dxl),
            (part.at[k, c, xr, g1], xfin.at[k, 0, g1], dxr),
            (part.at[k, c, xl, g0], xfin.at[k, 1, g0], dxl),
            (part.at[k, c, xr, g0], xfin.at[k, 0, g0], dxr),
            (part.at[k, c, xl, g1], xfin.at[k, 1, g1], dxl),
        ]
        return [
            remote(a, b, send.at[6], xrs.at[k, min(i, 2)], d) for i, (a, b, d) in enumerate(pairs)
        ]

    def add_mate(k, xx, g, extra=None):
        t = part[k, c, xx, g, :].astype(F32) + precv[k, xx, g, :].astype(F32)
        if extra is not None:
            t = t + extra.astype(F32)
        part[k, c, xx, g, :] = t.astype(BF)

    def send_sums(k):
        copies = spread(k)
        mate_copy(k).wait_recv()
        add_mate(k, xo, pl.ds(0, PC))
        add_mate(k, xr, g1)
        add_mate(k, xl, g0)
        for copy in copies[:4]:
            copy.start()

    def join_sums(k):
        copies = spread(k)
        copies[0].wait_recv()
        add_mate(k, xr, g0, xrelay[k, 0])
        copies[4].start()
        copies[1].wait_recv()
        add_mate(k, xl, g1, xrelay[k, 1])
        copies[5].start()

    def finish(k):
        remote(xfin.at[k], xfin.at[k], send.at[6], xrs.at[k, 2], dxr).wait_recv()
        total = part[k, c, x].astype(F32) + precv[k, x].astype(F32)
        total = total + xfin[k, 0].astype(F32) + xfin[k, 1].astype(F32)
        out[k * PC:(k + 1) * PC, :] = total.astype(BF)

    def row_lse(k):
        flat = jnp.transpose(lnat[...])
        mine = jnp.zeros((2, ROWS), F32)
        for i in range(NY):
            mine = jnp.where(y == i, flat[2 * i:2 * i + 2, :], mine)
        lse_ref[...] = mine * LN2

    def run(plan):
        for f, k in plan:
            with scope(f"{f.__name__}{k}"):
                f(k)

    last_keys(0, ())
    run(((send_stats, 0),))
    last_keys(1, ((send_shares, 0),))
    run(((send_stats, 1), (join_shares, 0)))
    last_keys(2, ((send_shares, 1), (merge, 0)))
    run((
        (send_stats, 2), (join_shares, 1), (send_shares, 2), (send_sums, 0), (merge, 1),
        (join_sums, 0), (join_shares, 2), (send_sums, 1), (merge, 2), (join_sums, 1),
        (send_sums, 2), (finish, 0), (row_lse, 0), (join_sums, 2), (finish, 1), (finish, 2),
    ))
    with scope("drain"):
        groups = (xbuf.at[pl.ds(0, 7)], kvb.at[pl.ds(0, 3)], qb.at[pl.ds(0, 3)],
                  stats.at[pl.ds(0, 3)], dbuf.at[pl.ds(0, 3)], precv, part.at[:, 0, pl.ds(0, 3)])
        for i, ref in enumerate(groups):
            remote(ref, ref, send.at[i], grs.at[0, 0], dm).wait_send()
        border.wait_send()


def tables():
    inverse = ROPE_BASE ** (-np.arange(HD // 2, dtype=np.float64) * 2.0 / HD)
    inverse = inverse.astype(np.float32).astype(np.float64)
    inverse = np.concatenate([inverse, inverse])
    place = np.arange(ROWS).reshape(2 * NX, NCH, PC).transpose(1, 0, 2).reshape(-1)
    local = place[:, None] * inverse[None, :]
    offset = (np.arange(NZ * NY) * ROWS)[:, None] * inverse[None, :]
    return [f(a).astype(np.float32) for a in (local, offset) for f in (np.cos, np.sin)]


DMA = pltpu.SemaphoreType.DMA


def per_device(
    tokens, norm_gain, w_query, w_key, w_value, w_outer, w_inner, w_signal,
    conv_taps, lambdas, head_gain, attend_proj, convolve_proj,
):
    rc, rs, oc, os_ = tables()
    v = pltpu.VMEM
    mixed, lse = pl.pallas_call(
        layer_kernel,
        out_shape=(
            jax.ShapeDtypeStruct((BLK, 2048), BF),
            jax.ShapeDtypeStruct((2, ROWS), F32),
        ),
        in_specs=[vmem(), pl.BlockSpec(memory_space=pltpu.SMEM)] + [vmem()] * 4 + [hbm()] * 11,
        out_specs=(vmem(), vmem()),
        scratch_shapes=[
            v((2 * NX, NCH, 2 * NX, PC, 256), BF), v((2048, HD), F32), v((ROWS, HD), F32), v((ROWS, HD), F32),
            v((6, 2048, 256), BF),
            v((256, 2048), BF), v((256, 2048), BF),
            v((ROWS + 8, 256), F32), v((ROWS, 256), F32), v((ROWS, 256), BF), v((ROWS, HD), F32),
            v((NY, ROWS, VD), BF), v((NZ, ROWS, 2 * VD), BF),
            v((2, NY, ROWS, HD), F32), v((2, NY, ROWS, HD), F32), v((2, NY, ROWS, VD), F32),
            v((ROWS, HD), F32), v((NY, NCH, 8, CH), F32), v((NY, ROWS, VD), BF),
            v((2, NCH * HF, VD), BF), v((2, ROWS, VD), BF),
            v((NCH, 2, NX, PC, 2048), BF), v((NCH, NX, PC, 2048), BF),
            v((NCH, 2, PC // 2, 2048), BF), v((NCH, 2, PC, 2048), BF),
            DMA((10,)), DMA((NCH,)), DMA((2,)), DMA((7,)), DMA((NCH, 5)), DMA((7,)), DMA((7,)),
            DMA((NCH,)), DMA((NCH, 3)), DMA((NCH,)), DMA((NCH, 3)),
        ],
        compiler_params=pltpu.CompilerParams(
            collective_id=1, has_side_effects=True, vmem_limit_bytes=62 * 2 ** 20
        ),
        name="layer",
    )(
        norm_gain.reshape(16, HD), lambdas, head_gain.reshape(1, -1), conv_taps, oc, os_,
        tokens.reshape(2 * NX, BLK, 256), rc, rs,
        w_query, w_key, w_value, w_outer, w_inner, w_signal, attend_proj, convolve_proj,
    )
    return mixed, lse.T


def solution(mesh):
    return jax.shard_map(
        per_device,
        mesh=mesh,
        in_specs=(
            P("sp", "tp"), P(), P(None, "tp"), P(None, "tp"), P(None, "tp"), P(None, "tp"),
            P(None, "tp"), P(None, "tp"), P(None, "tp"), P("tp"), P(), P("tp", None), P("tp", None),
        ),
        out_specs=(P(("sp", "tp"), None), P("sp", "tp")),
        check_vma=False,
    )
```

```python
import functools

import jax
import jax.numpy as jnp
import numpy as np
from jax import lax
from jax.experimental import pallas as pl
from jax.experimental.pallas import tpu as pltpu
from jax.sharding import PartitionSpec as P

MESH = pl.DeviceIdType.MESH
BF = jnp.bfloat16
F32 = jnp.float32
ROPE_BASE = 500000.0
NORM_EPS = 1e-05
HEAD_KEEP = 0.8
MASKED = -1e30
LOG2E = float(np.log2(np.e))
LN2 = float(np.log(2.0))
NZ, NY, NX = 4, 4, 4
ROWS = 768
HD = 128
VD = 256
CH = 256
NCH = ROWS // CH
HF = CH // 2
PC = 32
BLK = 96


def vmem():
    return pl.BlockSpec(memory_space=pltpu.VMEM)


def hbm():
    return pl.BlockSpec(memory_space=pl.ANY)


def remote(src, dst, ssem, rsem, dev):
    return pltpu.make_async_remote_copy(
        src_ref=src, dst_ref=dst, send_sem=ssem, recv_sem=rsem, device_id=dev, device_id_type=MESH
    )


def scope(name):
    return jax.named_scope(name)


def greet(devs):
    barrier = pltpu.get_barrier_semaphore()
    for dev in devs:
        pl.semaphore_signal(barrier, inc=1, device_id=dev, device_id_type=MESH)
    pl.semaphore_wait(barrier, len(devs))


def layer_kernel(
    gain, lam, hgain, taps, oc, os_, tok, rch, rsh, wq, wk, wv, wo, wi, ws, ap, cp,
    out, lse_ref,
    xbuf, gcol, rc, rs, wbuf, apb, cpb, prod, outer, conv, lnat,
    qb, kvb, m_ref, l_ref, acc, lt, stats, dbuf, relay, fin,
    part, precv, xrelay, xfin,
    wsem, tsem, bsem, send, grs, krs, qrs, trs, drs, prs, xrs,
):
    sp = lax.axis_index("sp")
    tp = lax.axis_index("tp")
    x, c = tp // 2, tp % 2
    z, y = sp // NY, sp % NY
    xr, xl, xo = lax.rem(x + 1, NX), lax.rem(x + 3, NX), lax.rem(x + 2, NX)
    yr, yl, yo = lax.rem(y + 1, NY), lax.rem(y + 3, NY), lax.rem(y + 2, NY)
    zr, zl, zo = lax.rem(z + 1, NZ), lax.rem(z + 3, NZ), lax.rem(z + 2, NZ)
    dxr, dxl, dm = (sp, xr * 2 + c), (sp, xl * 2 + c), (sp, x * 2 + (1 - c))
    dyr, dyl, dyo = (z * NY + yr, tp), (z * NY + yl, tp), (z * NY + yo, tp)
    dzr, dzl = (zr * NY + y, tp), (zl * NY + y, tp)
    dn, dp = (lax.rem(sp + 1, NZ * NY), tp), (lax.rem(sp + NZ * NY - 1, NZ * NY), tp)
    right, left, opp = xr * 2 + c, xl * 2 + c, xo * 2 + c

    tcopies = [
        pltpu.make_async_copy(tok.at[:, pl.ds(k * PC, PC), :], xbuf.at[tp, k], tsem.at[k])
        for k in range(NCH)
    ]
    for copy in tcopies:
        copy.start()
    weights = ((wk, wbuf.at[0]), (wv, wbuf.at[1]), (wq, wbuf.at[2]), (wi, wbuf.at[3]),
               (ws, wbuf.at[4]), (wo, wbuf.at[5]), (rch, rc), (rsh, rs), (ap, apb), (cp, cpb))
    wcopies = [pltpu.make_async_copy(a, b, wsem.at[i]) for i, (a, b) in enumerate(weights)]
    for copy in wcopies:
        copy.start()
    with scope("greet"):
        greet([dxr, dxl, dm, dyr, dyl, dyo, dzr, dzl, dn, dp])

    def go(copy):
        copy.start()

    def rows_of(k, h=None):
        return pl.ds(k * CH, CH) if h is None else pl.ds(k * CH + h * HF, HF)

    def pass_on(k, kind, block, h, dev):
        slot = (0, 1, 4, 2, 3, 4, 4, 4, 4)[kind]
        ref = xbuf.at[block, k] if h is None else xbuf.at[block, k, pl.ds(h * NX, NX)]
        return remote(ref, ref, send.at[0], grs.at[k, slot], dev)

    def send_own(k):
        tcopies[k].wait()
        go(pass_on(k, 0, tp, None, dxr))
        go(pass_on(k, 1, tp, None, dxl))
        go(pass_on(k, 2, tp, None, dm))

    def near(k):
        pass_on(k, 0, tp, None, dxr).wait_recv()
        go(pass_on(k, 3, left, 0, dxr))
        go(pass_on(k, 5, left, None, dm))
        pass_on(k, 1, tp, None, dxl).wait_recv()
        go(pass_on(k, 4, right, 1, dxl))
        go(pass_on(k, 6, right, None, dm))

    def far(k):
        pass_on(k, 3, left, 0, dxr).wait_recv()
        go(pass_on(k, 7, opp, 0, dm))
        pass_on(k, 4, right, 1, dxl).wait_recv()
        go(pass_on(k, 8, opp, 1, dm))

    def mates(k):
        ref = xbuf.at[pl.ds(0, NX), k]
        remote(ref, ref, send.at[0], grs.at[k, 4], dm).wait_recv()

    def ring(buf, me, lf, rt, ss, rs_, d_r, d_l):
        def one(block, k, h, kind, dev):
            ref = buf.at[block, rows_of(k, h)]
            return remote(ref, ref, ss, rs_.at[kind if kind == 6 else 2 * k + kind], dev)

        return [
            [one(me, k, None, 0, d_r), one(me, k, None, 1, d_l),
             one(lf, k, 0, 6, d_r), one(rt, k, 1, 6, d_l)]
            for k in range(NCH)
        ]

    kring = ring(kvb, z, zl, zr, send.at[1], krs, dzr, dzl)
    qring = ring(qb, y, yl, yr, send.at[2], qrs, dyr, dyl)

    def ring_send(copies):
        copies[0].start()
        copies[1].start()

    def ring_relay(copies):
        copies[0].wait_recv()
        copies[2].start()
        copies[1].wait_recv()
        copies[3].start()

    def ring_far(buf, sem, me, dev):
        remote(buf.at[me], buf.at[me], send.at[1], sem.at[6], dev).wait_recv()

    border = remote(prod.at[pl.ds(ROWS, 8)], prod.at[pl.ds(0, 8)], bsem.at[0], bsem.at[1], dn)
    co = oc[pl.ds(sp, 1), :]
    so = os_[pl.ds(sp, 1), :]

    def compute(k):
        rows = rows_of(k)
        square = jnp.zeros((CH, HD), F32)
        blocks = [xbuf[b, k].reshape(CH, 256) for b in range(2 * NX)]
        for xb in blocks:
            xf = xb.astype(F32)
            square += xf[:, :HD] * xf[:, :HD] + xf[:, HD:] * xf[:, HD:]
        wide = jnp.concatenate(blocks, axis=1)
        total = jnp.sum(square, axis=1, keepdims=True)
        inv = lax.rsqrt(total / (2 * NX * 256) + NORM_EPS)
        c_r, s_r = rc[rows, :], rs[rows, :]
        cosine = co * c_r - so * s_r
        sine = so * c_r + co * s_r
        lane = lax.broadcasted_iota(jnp.int32, (CH, HD), 1)
        sine = jnp.where(lane < HD // 2, -sine, sine)

        def project(i):
            return inv * jnp.dot(wide, wbuf[i], preferred_element_type=F32)

        def turn(v):
            parts = []
            for j in range(2):
                t = v[:, j * HD:(j + 1) * HD]
                parts.append(t * cosine + pltpu.roll(t, HD // 2, 1) * sine)
            return jnp.concatenate(parts, axis=1)

        kvb[z, rows, 0:VD] = turn(project(0)).astype(BF)
        kvb[z, rows, VD:2 * VD] = project(1).astype(BF)
        qb[y, rows, :] = (turn(project(2)) * (LOG2E * HD ** -0.5)).astype(BF)
        pr = project(3) * project(4)
        og = project(5)
        for t in range(2 * NX):
            at = t * BLK + k * PC
            prod[8 + at:8 + at + PC, :] = pr[t * PC:(t + 1) * PC]
            outer[at:at + PC, :] = og[t * PC:(t + 1) * PC]
        if k == NCH - 1:
            border.start()
        ring_send(kring[k])
        ring_send(qring[k])

    def scores(qi, kj, rows, j):
        q = qb[qi, rows, j * HD:(j + 1) * HD]
        k = kvb[kj, :, j * HD:(j + 1) * HD]
        return lax.dot_general(q, k, (((1,), (1,)), ((), ())), preferred_element_type=F32)

    def absorb(qi, kj, rows, j, s):
        before = m_ref[j, qi, rows, :]
        now = jnp.maximum(before, jnp.max(s, axis=1, keepdims=True))
        fade = jnp.exp2(before - now)
        p = jnp.exp2(s - jnp.concatenate([now] * (ROWS // HD), axis=1))
        total = l_ref[j, qi, rows, :] * fade
        for i in range(ROWS // HD):
            total = total + p[:, i * HD:(i + 1) * HD]
        l_ref[j, qi, rows, :] = total
        m_ref[j, qi, rows, :] = now
        acc[j, qi, rows, :] = acc[j, qi, rows, :] * jnp.concatenate([fade] * 2, axis=1) + jnp.dot(
            p.astype(BF), kvb[kj, :, VD:2 * VD], preferred_element_type=F32
        )

    def attend(qi, kj, rows, mask=None):
        ss = [scores(qi, kj, rows, j) for j in range(2)]
        for j in range(2):
            s = ss[j] if mask is None else jnp.where(mask, ss[j], MASKED)
            absorb(qi, kj, rows, j, s)

    def place(p):
        return ((p >> 5) & 7) * BLK + (p >> 8) * PC + (p & 31)

    def own_pair():
        row = place(lax.broadcasted_iota(jnp.int32, (ROWS, HD), 0))
        row = jnp.concatenate([row] * (ROWS // HD), axis=1)
        col = place(lax.broadcasted_iota(jnp.int32, (1, ROWS), 1))
        attend(y, z, pl.ds(0, ROWS), col <= row)

    def scale_weights():
        g = jnp.concatenate([gain[...], jnp.zeros((HD - 16, HD), F32)], axis=0)
        g = jnp.transpose(g)
        for b in range(16):
            gcol[b * HD:(b + 1) * HD, :] = jnp.broadcast_to(g[:, b:b + 1], (HD, HD))

        def one(i, _):
            for b in range(8):
                rows = slice(b * 256, (b + 1) * 256)
                col = gcol[rows, :]
                w = wbuf[i, rows, :].astype(F32)
                wbuf[i, rows, :] = (w * jnp.concatenate([col, col], axis=1)).astype(BF)
            return 0

        lax.fori_loop(0, 6, one, 0)

    def start():
        m_ref[...] = jnp.full(m_ref.shape, MASKED, F32)
        l_ref[...] = jnp.zeros(l_ref.shape, F32)
        acc[...] = jnp.zeros(acc.shape, F32)

    send_own(0)
    send_own(1)
    with scope("init"):
        start()
        for copy in wcopies:
            copy.wait()
    with scope("scale"):
        scale_weights()
    with scope("near0"):
        near(0)
    with scope("near1"):
        near(1)
    send_own(2)
    with scope("far0"):
        far(0)
    with scope("mates0"):
        mates(0)
    with scope("comp0"):
        compute(0)
    with scope("near2"):
        near(2)
    with scope("far1"):
        far(1)
    with scope("mates1"):
        mates(1)
    with scope("comp1"):
        compute(1)
    with scope("far2"):
        far(2)
    with scope("mates2"):
        mates(2)
    with scope("qrel0"):
        ring_relay(qring[0])
    with scope("comp2"):
        compute(2)
    with scope("own"):
        own_pair()
    with scope("conv"):
        border.wait_recv()

        @pl.when(sp == 0)
        def _():
            prod[0:8, :] = jnp.zeros((8, 256), F32)

        tv = taps[...].astype(F32)
        smoothed = (
            tv[0:1] * prod[6:6 + ROWS, :] + tv[1:2] * prod[7:7 + ROWS, :] + tv[2:3] * prod[8:8 + ROWS, :]
        )
        conv[...] = (outer[...] * smoothed).astype(BF)
    with scope("qrel1"):
        ring_relay(qring[1])
    with scope("rel0"):
        ring_relay(kring[0])
    with scope("qrel2"):
        ring_relay(qring[2])
    with scope("rel1"):
        ring_relay(kring[1])

    def step(i, _):
        @pl.when(i == 2)
        def _():
            with scope("qfar"):
                ring_far(qb, qrs, y, dyr)

        @pl.when(i == 3)
        def _():
            with scope("rel2"):
                ring_relay(kring[2])

        mine = i < 3
        turn_ = jnp.where(i == 0, 1, jnp.where(i == 1, 3, 2))
        qi = jnp.where(mine, lax.rem(y + turn_, NY), lax.rem(i + 1, NY))
        kj = jnp.where(mine, z, zl)
        need = (mine & (qi > y)) | (~mine & (z >= 1))

        @pl.when(need)
        def _():
            with scope("item"):
                attend(qi, kj, pl.ds(0, ROWS))

        return 0

    lax.fori_loop(0, 7, step, 0)
    lam_v = lam[0]

    def last_keys(k, between):
        def body(i, _):
            right_turn = i == 0
            if k == 0:
                @pl.when(i == 1)
                def _():
                    with scope("kfar"):
                        ring_far(kvb, krs, z, dzr)

            kj = jnp.where(right_turn, zr, zo)

            @pl.when((z == 3) | ((i == 1) & (z == 2)))
            def _():
                with scope("tiles"):
                    ss = [[scores(qi, kj, rows_of(k), j) for qi in range(NY)] for j in range(2)]
                    for j in range(2):
                        for qi in range(NY):
                            absorb(qi, kj, rows_of(k), j, ss[j][qi])

            if between:
                @pl.when(right_turn)
                def _():
                    for f, kk in between:
                        with scope(f"{f.__name__}{kk}"):
                            f(kk)

            return 0

        lax.fori_loop(0, 2, body, 0)

    def stat_copies(k):
        ref = stats.at[y, k]
        return [
            remote(ref, ref, send.at[3], trs.at[k], dev) for dev in (dyr, dyl, dyo)
        ]

    def send_stats(k):
        rows = rows_of(k)
        lane = lax.broadcasted_iota(jnp.int32, (CH, HD), 1)
        table = jnp.full((CH, HD), MASKED, F32)
        for qi in range(NY):
            for j in range(2):
                total = jnp.sum(l_ref[j, qi, rows, :], axis=1, keepdims=True)
                lse = m_ref[j, qi, rows, :] + jnp.log2(jnp.maximum(total, 1e-37))
                table = jnp.where(lane == 2 * qi + j, lse, table)
        stats[y, k] = jnp.transpose(table)[0:8, :]
        for copy in stat_copies(k):
            copy.start()

    def pick(rows, qi, j):
        lanes = lax.broadcasted_iota(jnp.int32, (CH, HD), 1)
        return jnp.sum(jnp.where(lanes == 2 * qi + j, lt[rows, :], 0.0), axis=1, keepdims=True)

    def share(rows, qi):
        outs = []
        for j in range(2):
            f = jnp.exp2(m_ref[j, qi, rows, :] - pick(rows, qi, j))
            outs.append(acc[j, qi, rows, :] * jnp.concatenate([f] * 2, axis=1))
        return outs[0] - lam_v * outs[1]

    def scatter(k):
        h0, h1 = rows_of(k, 0), rows_of(k, 1)
        at = pl.ds(k * HF, HF)
        pairs = [
            (dbuf.at[yo, h0], relay.at[0, at], dyr),
            (dbuf.at[yo, h1], relay.at[1, at], dyl),
            (dbuf.at[yr, h1], fin.at[0, h1], dyr),
            (dbuf.at[yl, h0], fin.at[1, h0], dyl),
            (dbuf.at[yr, h0], fin.at[0, h0], dyr),
            (dbuf.at[yl, h1], fin.at[1, h1], dyl),
        ]
        return [
            remote(a, b, send.at[4], drs.at[k, min(i, 2)], d) for i, (a, b, d) in enumerate(pairs)
        ]

    def send_shares(k):
        rows = rows_of(k)
        ref = stats.at[pl.ds(0, NY - 1), k]
        remote(ref, ref, send.at[3], trs.at[k], dyr).wait_recv()
        parts = [stats[i, k] for i in range(NY)]
        peak = jnp.maximum(jnp.maximum(parts[0], parts[1]), jnp.maximum(parts[2], parts[3]))
        whole = peak + jnp.log2(sum(jnp.exp2(p - peak) for p in parts))
        lt[rows, :] = jnp.transpose(jnp.concatenate([whole, jnp.zeros((HD - 8, CH), F32)], axis=0))

        def one(i, _):
            qi = lax.rem(y + jnp.where(i == 0, 2, jnp.where(i == 1, 1, 3)), NY)
            dbuf[qi, rows, :] = share(rows, qi).astype(BF)
            return 0

        lax.fori_loop(0, NY - 1, one, 0)
        for copy in scatter(k)[:4]:
            copy.start()

    def join_shares(k):
        copies = scatter(k)
        h0, h1 = rows_of(k, 0), rows_of(k, 1)
        at = pl.ds(k * HF, HF)
        copies[0].wait_recv()
        dbuf[yr, h0, :] = (dbuf[yr, h0, :].astype(F32) + relay[0, at, :].astype(F32)).astype(BF)
        copies[4].start()
        copies[1].wait_recv()
        dbuf[yl, h1, :] = (dbuf[yl, h1, :].astype(F32) + relay[1, at, :].astype(F32)).astype(BF)
        copies[5].start()

    def mate_copy(k):
        return remote(part.at[k, 1 - c], precv.at[k], send.at[5], prs.at[k], dm)

    def merge(k):
        rows = rows_of(k)
        ref = fin.at[:, rows]
        remote(ref, ref, send.at[4], drs.at[k, 2], dyr).wait_recv()
        d = share(rows, y) + fin[0, rows, :].astype(F32) + fin[1, rows, :].astype(F32)
        back = lax.rsqrt(jnp.mean(d * d, axis=1, keepdims=True) + NORM_EPS)
        att = (d * back * hgain[...] * HEAD_KEEP).astype(BF)
        pieces = [slice(t * BLK + k * PC, t * BLK + (k + 1) * PC) for t in range(2 * NX)]
        for t in range(2 * NX):
            lnat[pieces[t], :] = lt[k * CH + t * PC:k * CH + (t + 1) * PC, :]
        con = jnp.concatenate([conv[pieces[t], :] for t in range(2 * NX)], axis=0)
        cols = 512
        for n in range(2048 // cols):
            cs = slice(n * cols, (n + 1) * cols)
            p = jnp.dot(att, apb[:, cs], preferred_element_type=F32) + jnp.dot(
                con, cpb[:, cs], preferred_element_type=F32
            )
            p = p.astype(BF)
            for t in range(2 * NX):
                part[k, t % 2, t // 2, :, cs] = p[t * PC:(t + 1) * PC]
        mate_copy(k).start()

    g0, g1 = pl.ds(0, PC // 2), pl.ds(PC // 2, PC // 2)

    def spread(k):
        pairs = [
            (part.at[k, c, xo, g0], xrelay.at[k, 0], dxr),
            (part.at[k, c, xo, g1], xrelay.at[k, 1], dxl),
            (part.at[k, c, xr, g1], xfin.at[k, 0, g1], dxr),
            (part.at[k, c, xl, g0], xfin.at[k, 1, g0], dxl),
            (part.at[k, c, xr, g0], xfin.at[k, 0, g0], dxr),
            (part.at[k, c, xl, g1], xfin.at[k, 1, g1], dxl),
        ]
        return [
            remote(a, b, send.at[6], xrs.at[k, min(i, 2)], d) for i, (a, b, d) in enumerate(pairs)
        ]

    def add_mate(k, xx, g, extra=None):
        t = part[k, c, xx, g, :].astype(F32) + precv[k, xx, g, :].astype(F32)
        if extra is not None:
            t = t + extra.astype(F32)
        part[k, c, xx, g, :] = t.astype(BF)

    def send_sums(k):
        copies = spread(k)
        mate_copy(k).wait_recv()
        add_mate(k, xo, pl.ds(0, PC))
        add_mate(k, xr, g1)
        add_mate(k, xl, g0)
        for copy in copies[:4]:
            copy.start()

    def join_sums(k):
        copies = spread(k)
        copies[0].wait_recv()
        add_mate(k, xr, g0, xrelay[k, 0])
        copies[4].start()
        copies[1].wait_recv()
        add_mate(k, xl, g1, xrelay[k, 1])
        copies[5].start()

    def finish(k):
        remote(xfin.at[k], xfin.at[k], send.at[6], xrs.at[k, 2], dxr).wait_recv()
        total = part[k, c, x].astype(F32) + precv[k, x].astype(F32)
        total = total + xfin[k, 0].astype(F32) + xfin[k, 1].astype(F32)
        out[k * PC:(k + 1) * PC, :] = total.astype(BF)

    def row_lse(k):
        flat = jnp.transpose(lnat[...])
        mine = jnp.zeros((2, ROWS), F32)
        for i in range(NY):
            mine = jnp.where(y == i, flat[2 * i:2 * i + 2, :], mine)
        lse_ref[...] = mine * LN2

    def run(plan):
        for f, k in plan:
            with scope(f"{f.__name__}{k}"):
                f(k)

    last_keys(0, ())
    run(((send_stats, 0),))
    last_keys(1, ((send_shares, 0),))
    run(((send_stats, 1), (join_shares, 0)))
    last_keys(2, ((send_shares, 1),))
    run((
        (send_stats, 2), (join_shares, 1), (merge, 0), (send_shares, 2), (send_sums, 0), (merge, 1),
        (join_sums, 0), (join_shares, 2), (send_sums, 1), (merge, 2), (join_sums, 1),
        (send_sums, 2), (finish, 0), (row_lse, 0), (join_sums, 2), (finish, 1), (finish, 2),
    ))
    with scope("drain"):
        groups = (xbuf.at[pl.ds(0, 7)], kvb.at[pl.ds(0, 3)], qb.at[pl.ds(0, 3)],
                  stats.at[pl.ds(0, 3)], dbuf.at[pl.ds(0, 3)], precv, part.at[:, 0, pl.ds(0, 3)])
        for i, ref in enumerate(groups):
            remote(ref, ref, send.at[i], grs.at[0, 0], dm).wait_send()
        border.wait_send()


def tables():
    inverse = ROPE_BASE ** (-np.arange(HD // 2, dtype=np.float64) * 2.0 / HD)
    inverse = inverse.astype(np.float32).astype(np.float64)
    inverse = np.concatenate([inverse, inverse])
    place = np.arange(ROWS).reshape(2 * NX, NCH, PC).transpose(1, 0, 2).reshape(-1)
    local = place[:, None] * inverse[None, :]
    offset = (np.arange(NZ * NY) * ROWS)[:, None] * inverse[None, :]
    return [f(a).astype(np.float32) for a in (local, offset) for f in (np.cos, np.sin)]


DMA = pltpu.SemaphoreType.DMA


def per_device(
    tokens, norm_gain, w_query, w_key, w_value, w_outer, w_inner, w_signal,
    conv_taps, lambdas, head_gain, attend_proj, convolve_proj,
):
    rc, rs, oc, os_ = tables()
    v = pltpu.VMEM
    mixed, lse = pl.pallas_call(
        layer_kernel,
        out_shape=(
            jax.ShapeDtypeStruct((BLK, 2048), BF),
            jax.ShapeDtypeStruct((2, ROWS), F32),
        ),
        in_specs=[vmem(), pl.BlockSpec(memory_space=pltpu.SMEM)] + [vmem()] * 4 + [hbm()] * 11,
        out_specs=(vmem(), vmem()),
        scratch_shapes=[
            v((2 * NX, NCH, 2 * NX, PC, 256), BF), v((2048, HD), F32), v((ROWS, HD), F32), v((ROWS, HD), F32),
            v((6, 2048, 256), BF),
            v((256, 2048), BF), v((256, 2048), BF),
            v((ROWS + 8, 256), F32), v((ROWS, 256), F32), v((ROWS, 256), BF), v((ROWS, HD), F32),
            v((NY, ROWS, VD), BF), v((NZ, ROWS, 2 * VD), BF),
            v((2, NY, ROWS, HD), F32), v((2, NY, ROWS, HD), F32), v((2, NY, ROWS, VD), F32),
            v((ROWS, HD), F32), v((NY, NCH, 8, CH), F32), v((NY, ROWS, VD), BF),
            v((2, NCH * HF, VD), BF), v((2, ROWS, VD), BF),
            v((NCH, 2, NX, PC, 2048), BF), v((NCH, NX, PC, 2048), BF),
            v((NCH, 2, PC // 2, 2048), BF), v((NCH, 2, PC, 2048), BF),
            DMA((10,)), DMA((NCH,)), DMA((2,)), DMA((7,)), DMA((NCH, 5)), DMA((7,)), DMA((7,)),
            DMA((NCH,)), DMA((NCH, 3)), DMA((NCH,)), DMA((NCH, 3)),
        ],
        compiler_params=pltpu.CompilerParams(
            collective_id=1, has_side_effects=True, vmem_limit_bytes=62 * 2 ** 20
        ),
        name="layer",
    )(
        norm_gain.reshape(16, HD), lambdas, head_gain.reshape(1, -1), conv_taps, oc, os_,
        tokens.reshape(2 * NX, BLK, 256), rc, rs,
        w_query, w_key, w_value, w_outer, w_inner, w_signal, attend_proj, convolve_proj,
    )
    return mixed, lse.T


def solution(mesh):
    return jax.shard_map(
        per_device,
        mesh=mesh,
        in_specs=(
            P("sp", "tp"), P(), P(None, "tp"), P(None, "tp"), P(None, "tp"), P(None, "tp"),
            P(None, "tp"), P(None, "tp"), P(None, "tp"), P("tp"), P(), P("tp", None), P("tp", None),
        ),
        out_specs=(P(("sp", "tp"), None), P("sp", "tp")),
        check_vma=False,
    )
```
